32 devices in a mesh: sp: 8 (over z, x), tp: 4 (over y, core).
Axes of the slice: x: 2, y: 2, z: 4, core: 2. Of those that a mesh axis runs over, the one named last changes fastest.
Arguments:
- residual_in: bfloat16 [1024, 2048], P('sp', 'tp'), may hold values from -8 to 8
- query_alpha: bfloat16 [1024, 2048], P('sp', 'tp'), may hold values from -8 to 8
- pairs_alpha: bfloat16 [1024, 16, 128], P('sp', 'tp'), may hold values from -8 to 8
- offset_alpha: float32 [1024, 32], P('sp', 'tp'), may hold values from -18 to -1
- gain_alpha: float32 [2048], P('tp'), may hold values from 0.1 to 1.9
- query_beta: bfloat16 [1024, 2048], P('sp', 'tp'), may hold values from -8 to 8
- pairs_beta: bfloat16 [1024, 16, 256], P('sp', 'tp'), may hold values from -8 to 8
- offset_beta: float32 [1024, 16], P('sp', 'tp'), may hold values from -18 to -1
- gain_beta: float32 [2048], P('tp'), may hold values from 0.1 to 1.9
- project_alpha: bfloat16 [2048, 2048], P('tp'), may hold values from -0.09375 to 0.09375
- project_beta: bfloat16 [2048, 2048], P('tp'), may hold values from -0.09375 to 0.09375
- gain_settle: float32 [2048], P('tp'), may hold values from 0 to 4
- bias_settle: float32 [2048], P('tp'), may hold values from -2.5 to 2.5
- expert_ids: int32 [1024, 2], P('sp'), may hold values from 0 to 7, as said below
- route_weight: float32 [1024, 2], P('sp'), may hold values from 0.1 to 0.9
- expert_gate: bfloat16 [8, 2048, 4096], P('sp', None, 'tp'), may hold values from -0.125 to 0.125
- expert_up: bfloat16 [8, 2048, 4096], P('sp', None, 'tp'), may hold values from -0.125 to 0.125
- expert_down: bfloat16 [8, 4096, 2048], P('sp', 'tp'), may hold values from -0.1875 to 0.1875
- gain_final: float32 [2048], P('tp'), may hold values from 0.1 to 1.9
- bias_final: float32 [2048], P('tp'), may hold values from -2.5 to 2.5
Outputs:
- layer_out: bfloat16 [1024, 2048], P('sp', 'tp')
The draws below stay inside these ranges and needn't reach their ends.
Inputs may be any that keep to these rules, and one draw needn't show every extreme that they name: `expert_ids`: the two numbers of a row differ and lie in one group of 2 consecutive experts. Among the rows of one device, no expert is named more than 48 times, and every expert of one group, the same group for all devices, is named exactly 48 times.
All inputs are finite; a program needn't handle non-finite values.
Results may differ from the reference program's by a relative error of at most 0.018.
Values may be sent and summed in bfloat16 or wider, within the bound.
No kernel may reach another device: no remote copies, remote signals or barrier semaphores. Data moves between devices by JAX's collectives and lax.ppermute only.
A program may use at most 64 MiB of HBM per device.

```python
import math
import jax
import jax.numpy as jnp
from jax import lax

D = 2048
HA = 32
DA = 64
HKA = 16
HB = 16
DB = 128
FFE = 4096
GROUPS = 4
TOK_DEV = 128
TOKEN_COUNT = 1024
EXPERTS = 8
EPG = 2
CAP = 48
HEAVY = 48
N_SP = 8
N_TP = 4


def rising(count, top):
    return top ** (jnp.arange(count, dtype=jnp.float32) / (count - 1))


def draw_residual_in(key, part):
    stream = jax.random.fold_in(key, 11)
    anchor_figure = jnp.clip(jax.random.normal(stream, (TOKEN_COUNT, D), jnp.float32), -4.0, 4.0)
    scale = rising(D, 3.0) / 1.7
    return (anchor_figure * scale[None, :]).astype(jnp.bfloat16)


def pair_draw(key, heads, width):
    first, second = jax.random.split(key)
    keys = 1.6 * jnp.clip(jax.random.normal(first, (TOKEN_COUNT, heads, width), jnp.float32), -4.0, 4.0)
    values = jnp.clip(jax.random.normal(second, (TOKEN_COUNT, heads, width), jnp.float32), -4.0, 4.0)
    values = values * (rising(heads, 3.0) / 1.7)[None, :, None]
    return jnp.concatenate([keys, values], axis=2).astype(jnp.bfloat16)


def draw_pairs_alpha(key, part):
    return pair_draw(jax.random.fold_in(key, 21), HKA, DA)


def draw_pairs_beta(key, part):
    return pair_draw(jax.random.fold_in(key, 22), HB, DB)


def offset_draw(key, heads):
    streams = jax.random.split(key, 7)
    blocks = TOKEN_COUNT // TOK_DEV
    share = 0.5
    fast = jax.random.uniform(streams[0], (heads,), jnp.float32) < share
    slow_base = -math.log(TOKEN_COUNT) - 3.3 - jax.random.uniform(streams[1], (heads,), jnp.float32, 0.5, 2.5)
    fast_base = -math.log(40.0) - 3.3 + jax.random.uniform(streams[2], (heads,), jnp.float32, -0.5, 0.5)
    anchor_figure = jnp.where(fast, fast_base, slow_base)
    slope_figure = jnp.repeat(jax.random.uniform(streams[3], (blocks, heads), jnp.float32, -0.7, 0.7), TOK_DEV, axis=0)
    coarse_estimate = jax.random.uniform(streams[4], (TOKEN_COUNT, heads), jnp.float32, -0.4, 0.4)
    marked_places = jax.random.randint(streams[5], (3, heads), 1, TOKEN_COUNT)
    sudden_jump_figure = jnp.any(jnp.arange(TOKEN_COUNT)[:, None, None] == marked_places[None, :, :], axis=1)
    dominant_figure = jax.random.uniform(streams[6], (TOKEN_COUNT, heads), jnp.float32, -2.5, -1.0)
    return jnp.where(sudden_jump_figure, dominant_figure, anchor_figure[None, :] + slope_figure + coarse_estimate).astype(jnp.float32)


def draw_offset_alpha(key, part):
    return offset_draw(jax.random.fold_in(key, 31), HA)


def draw_offset_beta(key, part):
    return offset_draw(jax.random.fold_in(key, 32), HB)


def draw_gain_settle(key, part):
    stream = jax.random.fold_in(key, 41)
    anchor_figure = 1.0 + 0.18 * jax.random.uniform(stream, (D,), jnp.float32, -1.0, 1.0)
    scale = rising(D, 3.0) / 1.7
    return (anchor_figure * scale).astype(jnp.float32)


def draw_expert_ids(key, part):
    blocks = TOKEN_COUNT // TOK_DEV
    heavy_group = jax.random.randint(jax.random.fold_in(key, 51), (), 0, GROUPS)

    def one_block(block_key):
        streams = jax.random.split(block_key, 5)
        rank = jax.random.permutation(streams[0], TOK_DEV)
        offset = jax.random.randint(streams[1], (GROUPS,), 0, EPG)
        stride = jax.random.randint(streams[2], (GROUPS,), 1, EPG)
        rotate = jax.random.randint(streams[3], (), 0, GROUPS - 1)
        flip = jax.random.randint(streams[4], (TOK_DEV,), 0, 2)
        in_heavy = rank < HEAVY
        rest = rank - HEAVY
        other = (heavy_group + 1 + (rest % (GROUPS - 1) + rotate) % (GROUPS - 1)) % GROUPS
        group = jnp.where(in_heavy, heavy_group, other)
        index = jnp.where(in_heavy, rank, rest // (GROUPS - 1))
        lead = group * EPG + (offset[group] + index) % EPG
        trail = group * EPG + (offset[group] + index + stride[group]) % EPG
        left = jnp.where(flip == 1, trail, lead)
        right = jnp.where(flip == 1, lead, trail)
        return jnp.stack([left, right], axis=1)
    ids = jax.vmap(one_block)(jax.random.split(jax.random.fold_in(key, 52), blocks))
    return ids.reshape(TOKEN_COUNT, 2).astype(jnp.int32)


def shard_levels(own_key, shape, shards, low, largest):
    def one(position, blocks):
        heights = jax.random.uniform(jax.random.fold_in(jax.random.fold_in(own_key, 6), position), (blocks,), jnp.float32, low / len(shards), largest / len(shards))
        return jnp.repeat(jnp.exp(heights), shape[position] // blocks).reshape((-1,) + (1,) * (len(shape) - position - 1))

    level = one(*shards[0])
    for cut in shards[1:]:
        level = level * one(*cut)
    return level


def noise(own_key, extent, deviation, most, cuts=(), kind=jnp.bfloat16):
    drawn = deviation * jax.random.normal(own_key, extent, jnp.float32)
    if cuts:
        drawn = drawn * shard_levels(own_key, extent, cuts, -0.22, 0.18)
    return jnp.clip(drawn, -most, most).astype(kind)


def setup_inputs(seed: int = 0) -> dict:
    arg_keys = jax.random.split(jax.random.key(seed), 21)
    residual_in = draw_residual_in(jax.random.fold_in(arg_keys[20], 71), 0)
    query_alpha = noise(arg_keys[1], (TOKEN_COUNT, HA * DA), 1.6, 8.0, ((0, 8), (1, 4)))
    pairs_alpha = draw_pairs_alpha(jax.random.fold_in(arg_keys[20], 71), 0)
    offset_alpha = draw_offset_alpha(jax.random.fold_in(arg_keys[20], 71), 0)
    gain_alpha = jnp.clip(1.0 + 0.18 * jax.random.normal(arg_keys[4], (HA * DA,), jnp.float32), 0.1, 1.9)
    query_beta = noise(arg_keys[5], (TOKEN_COUNT, HB * DB), 1.6, 8.0, ((0, 8), (1, 4)))
    pairs_beta = draw_pairs_beta(jax.random.fold_in(arg_keys[20], 71), 0)
    offset_beta = draw_offset_beta(jax.random.fold_in(arg_keys[20], 71), 0)
    gain_beta = jnp.clip(1.0 + 0.18 * jax.random.normal(arg_keys[8], (HB * DB,), jnp.float32), 0.1, 1.9)
    project_alpha = noise(arg_keys[9], (HA * DA, D), (HA * DA + HB * DB) ** -0.5, 0.09375, ((0, 4),))
    project_beta = noise(arg_keys[10], (HB * DB, D), (HA * DA + HB * DB) ** -0.5, 0.09375, ((0, 4),))
    gain_settle = draw_gain_settle(jax.random.fold_in(arg_keys[20], 71), 0)
    bias_settle = noise(arg_keys[12], (D,), 0.5, 2.5, ((0, 4),), jnp.float32)
    expert_ids = draw_expert_ids(jax.random.fold_in(arg_keys[20], 71), 0)
    route_weight = jnp.clip(0.1 + 0.79999997 * jax.random.uniform(arg_keys[14], (TOKEN_COUNT, 2), jnp.float32) ** shard_levels(arg_keys[14], (TOKEN_COUNT, 2), ((0, 8),), -0.2, 0.2), 0.1, 0.9)
    expert_gate = noise(arg_keys[15], (EXPERTS, D, FFE), D ** -0.5, 0.125, ((0, 8), (2, 4)))
    expert_up = noise(arg_keys[16], (EXPERTS, D, FFE), D ** -0.5, 0.125, ((0, 8), (2, 4)))
    expert_down = noise(arg_keys[17], (EXPERTS, FFE, D), (FFE // 4) ** -0.5, 0.1875, ((0, 8), (1, 4)))
    gain_final = jnp.clip(1.0 + 0.18 * jax.random.normal(arg_keys[18], (D,), jnp.float32), 0.1, 1.9)
    bias_final = noise(arg_keys[19], (D,), 0.5, 2.5, ((0, 4),), jnp.float32)
    return dict(residual_in=residual_in, query_alpha=query_alpha, pairs_alpha=pairs_alpha, offset_alpha=offset_alpha, gain_alpha=gain_alpha, query_beta=query_beta, pairs_beta=pairs_beta, offset_beta=offset_beta, gain_beta=gain_beta, project_alpha=project_alpha, project_beta=project_beta, gain_settle=gain_settle, bias_settle=bias_settle, expert_ids=expert_ids, route_weight=route_weight, expert_gate=expert_gate, expert_up=expert_up, expert_down=expert_down, gain_final=gain_final, bias_final=bias_final)


depth_scale = 2.0 ** 0.5
norm_eps = 1e-05

def stick_heads(queries, pairs, offsets, heads, kv_heads, width):
    share = heads // kv_heads
    q_heads = jnp.transpose(queries.reshape(TOKEN_COUNT, heads, width), (1, 0, 2))
    k_heads = jnp.transpose(pairs[:, :, :width], (1, 0, 2))
    v_heads = jnp.transpose(pairs[:, :, width:], (1, 0, 2))
    scale = width ** (-0.5)
    key_pos = jnp.arange(TOKEN_COUNT, dtype=jnp.int32)
    firsts = jnp.arange(TOKEN_COUNT // TOK_DEV, dtype=jnp.int32) * TOK_DEV

    def one_head(args):
        q_all, bias, index = args
        keys = k_heads[index // share]
        values = v_heads[index // share]
        blocks = q_all.reshape(TOKEN_COUNT // TOK_DEV, TOK_DEV, width)

        def one_block(inner):
            q_rows, first = inner
            scores = jnp.dot(q_rows, keys.T, preferred_element_type=jnp.float32) * scale + bias[None, :]
            query_pos = first + jnp.arange(TOK_DEV, dtype=jnp.int32)
            valid = key_pos[None, :] < query_pos[:, None]
            soft = jnp.where(valid, jax.nn.softplus(scores), 0.0)
            later = lax.cumsum(soft, axis=1, reverse=True) - soft
            weights = jnp.where(valid, jnp.exp(jax.nn.log_sigmoid(scores) - later), 0.0).astype(jnp.bfloat16)
            return jnp.dot(weights, values, preferred_element_type=jnp.float32)
        return lax.map(one_block, (blocks, firsts)).reshape(TOKEN_COUNT, width)
    out = lax.map(one_head, (q_heads, jnp.transpose(offsets), jnp.arange(heads, dtype=jnp.int32)))
    return jnp.transpose(out, (1, 0, 2)).reshape(TOKEN_COUNT, heads * width)

def group_norm(attend, gain):
    mean_sq = lax.optimization_barrier(jnp.mean(attend * attend, axis=1, keepdims=True))
    return (attend * lax.rsqrt(mean_sq + norm_eps) * gain).astype(jnp.bfloat16)

def shard_sum(products, count):

    def add_piece(total, index):
        term = jnp.zeros((count, D), jnp.float32)
        for left, right in products:
            width = left.shape[1] // N_TP
            piece = lax.dynamic_slice_in_dim(left, index * width, width, 1)
            block = lax.dynamic_slice_in_dim(right, index * width, width, 0)
            term = term + jnp.dot(piece, block, preferred_element_type=jnp.float32)
        rounded = lax.optimization_barrier(term.astype(jnp.bfloat16))
        return (total + rounded.astype(jnp.float32), None)
    total, _ = lax.scan(add_piece, jnp.zeros((count, D), jnp.float32), jnp.arange(N_TP, dtype=jnp.int32))
    return total

def layer_norm(total, gain, bias):
    mean = lax.optimization_barrier(jnp.sum(total, axis=1, keepdims=True)) / D
    var = lax.optimization_barrier(jnp.sum(total * total, axis=1, keepdims=True)) / D - mean * mean
    return ((total - mean) * lax.rsqrt(var + norm_eps) * gain + bias).astype(jnp.bfloat16)

def reference(residual_in, query_alpha, pairs_alpha, offset_alpha, gain_alpha, query_beta, pairs_beta, offset_beta, gain_beta, project_alpha, project_beta, gain_settle, bias_settle, expert_ids, route_weight, expert_gate, expert_up, expert_down, gain_final, bias_final):
    attend_alpha = stick_heads(query_alpha, pairs_alpha, offset_alpha, HA, HKA, DA)
    attend_beta = stick_heads(query_beta, pairs_beta, offset_beta, HB, HB, DB)
    normed_alpha = group_norm(attend_alpha, gain_alpha)
    normed_beta = group_norm(attend_beta, gain_beta)
    mixed = shard_sum(((normed_alpha, project_alpha), (normed_beta, project_beta)), TOKEN_COUNT).astype(jnp.bfloat16)
    first = depth_scale * residual_in.astype(jnp.float32) + mixed.astype(jnp.float32)
    settled = layer_norm(first, gain_settle, bias_settle)
    ids = expert_ids.reshape(N_SP, 2 * TOK_DEV)
    onehot = (ids[:, :, None] == jnp.arange(EXPERTS, dtype=jnp.int32)[None, None, :]).astype(jnp.int32)
    before = jnp.cumsum(onehot, axis=1, dtype=jnp.int32) - onehot
    slot = lax.optimization_barrier(jnp.sum(before * onehot, axis=2, dtype=jnp.int32))
    place = (jnp.arange(N_SP, dtype=jnp.int32)[:, None] * CAP + slot).reshape(TOKEN_COUNT * 2)
    owner = jnp.arange(TOKEN_COUNT * 2, dtype=jnp.int32) // 2
    table = jnp.full((EXPERTS, N_SP * CAP), TOKEN_COUNT, jnp.int32).at[expert_ids.reshape(TOKEN_COUNT * 2), place].set(owner)
    padded = jnp.concatenate([settled, jnp.zeros((1, D), jnp.bfloat16)], axis=0)

    def one_expert(args):
        rows, gate_w, up_w, down_w = args
        inputs = padded[rows]
        gate = jnp.dot(inputs, gate_w, preferred_element_type=jnp.float32)
        up = jnp.dot(inputs, up_w, preferred_element_type=jnp.float32)
        hidden = (jax.nn.silu(gate) * up).astype(jnp.bfloat16)
        return shard_sum(((hidden, down_w),), N_SP * CAP).astype(jnp.bfloat16)
    outputs = lax.map(one_expert, (table, expert_gate, expert_up, expert_down))
    picked = outputs[expert_ids, place.reshape(TOKEN_COUNT, 2)].astype(jnp.float32)
    routed = route_weight[:, 0:1] * picked[:, 0] + route_weight[:, 1:2] * picked[:, 1]
    second = depth_scale * settled.astype(jnp.float32) + routed
    return layer_norm(second, gain_final, bias_final)
```

```python
import jax
import jax.numpy as jnp
from jax import lax
from jax.experimental import pallas as pl
from jax.experimental.pallas import tpu as pltpu
from jax.sharding import PartitionSpec as P

depth_scale = 2.0**0.5
norm_eps = 1e-05


def break_block(acc, remain, queries, pairs, offsets, key_first, query_first):
    width = queries.shape[3]
    keys = pairs[:, :, :width]
    values = pairs[:, :, width:]
    length = offsets.shape[0]
    kv_heads = queries.shape[1]
    share = queries.shape[2]
    scores = jnp.einsum(
        "qhrd,khd->hrqk", queries, keys, preferred_element_type=jnp.float32
    ) * width ** (-0.5)
    scores = (
        scores + jnp.transpose(offsets.reshape(length, kv_heads, share), (1, 2, 0))[:, :, None, :]
    )
    query_pos = query_first + jnp.arange(queries.shape[0], dtype=jnp.int32)
    key_pos = key_first + jnp.arange(length, dtype=jnp.int32)
    valid = key_pos[None, :] < query_pos[:, None]
    soft = jnp.where(valid, jax.nn.softplus(scores), 0.0)
    later = lax.cumsum(soft, axis=3, reverse=True) - soft
    weights = jnp.where(
        valid, jnp.exp(jax.nn.log_sigmoid(scores) - later + remain[..., None]), 0.0
    ).astype(jnp.bfloat16)
    acc = acc + jnp.einsum("hrqk,khd->qhrd", weights, values, preferred_element_type=jnp.float32)
    return (acc, remain - jnp.sum(soft, axis=3))


def finish_norm(total, sums, gain, bias, columns):
    mean = sums[0] / columns
    var = sums[1] / columns - mean * mean
    return ((total - mean[:, None]) * lax.rsqrt(var + norm_eps)[:, None] * gain + bias).astype(
        jnp.bfloat16
    )


def general_body(
    residual_in,
    query_alpha,
    pairs_alpha,
    offset_alpha,
    gain_alpha,
    query_beta,
    pairs_beta,
    offset_beta,
    gain_beta,
    project_alpha,
    project_beta,
    gain_settle,
    bias_settle,
    expert_ids,
    route_weight,
    expert_gate,
    expert_up,
    expert_down,
    gain_final,
    bias_final,
):
    rows = residual_in.shape[0]
    mine = lax.axis_index("sp")
    count = lax.axis_size("sp")
    heads_tp = lax.axis_size("tp")
    width_alpha = pairs_alpha.shape[2] // 2
    width_beta = pairs_beta.shape[2] // 2
    grouped_alpha = query_alpha.reshape(rows, pairs_alpha.shape[1], -1, width_alpha)
    grouped_beta = query_beta.reshape(rows, pairs_beta.shape[1], -1, width_beta)
    query_first = mine * rows
    initial = (
        jnp.zeros(grouped_alpha.shape, jnp.float32),
        jnp.zeros(grouped_beta.shape, jnp.float32),
        jnp.zeros((grouped_alpha.shape[1], grouped_alpha.shape[2], rows), jnp.float32),
        jnp.zeros((grouped_beta.shape[1], grouped_beta.shape[2], rows), jnp.float32),
    )

    def visit(state, pairs, offsets, key_first):
        acc_alpha, acc_beta, rest_alpha, rest_beta = state
        acc_alpha, rest_alpha = break_block(
            acc_alpha, rest_alpha, grouped_alpha, pairs[0], offsets[0], key_first, query_first
        )
        acc_beta, rest_beta = break_block(
            acc_beta, rest_beta, grouped_beta, pairs[1], offsets[1], key_first, query_first
        )
        return (acc_alpha, acc_beta, rest_alpha, rest_beta)

    def maybe_visit(state, turn, pairs, offsets):
        return lax.cond(
            turn <= mine,
            lambda kept: visit(kept, pairs, offsets, (mine - turn) * rows),
            lambda kept: kept,
            state,
        )

    pairs_all = (
        lax.all_gather(pairs_alpha, "sp", axis=0, tiled=True),
        lax.all_gather(pairs_beta, "sp", axis=0, tiled=True),
    )
    offsets_all = (
        lax.all_gather(offset_alpha, "sp", axis=0, tiled=True),
        lax.all_gather(offset_beta, "sp", axis=0, tiled=True),
    )

    def turn_all(turn, state):
        first_row = (mine - turn) * rows
        pairs = (
            lax.dynamic_slice_in_dim(pairs_all[0], first_row, rows, 0),
            lax.dynamic_slice_in_dim(pairs_all[1], first_row, rows, 0),
        )
        offsets = (
            lax.dynamic_slice_in_dim(offsets_all[0], first_row, rows, 0),
            lax.dynamic_slice_in_dim(offsets_all[1], first_row, rows, 0),
        )
        return maybe_visit(state, turn, pairs, offsets)

    state = lax.fori_loop(0, count, turn_all, initial)
    attend_alpha = state[0].reshape(rows, -1)
    attend_beta = state[1].reshape(rows, -1)
    squares = lax.psum(
        (jnp.sum(attend_alpha * attend_alpha, axis=1), jnp.sum(attend_beta * attend_beta, axis=1)),
        "tp",
    )
    scale_alpha = lax.rsqrt(squares[0] / (attend_alpha.shape[1] * heads_tp) + norm_eps)
    scale_beta = lax.rsqrt(squares[1] / (attend_beta.shape[1] * heads_tp) + norm_eps)
    normed_alpha = (attend_alpha * scale_alpha[:, None] * gain_alpha).astype(jnp.bfloat16)
    normed_beta = (attend_beta * scale_beta[:, None] * gain_beta).astype(jnp.bfloat16)
    term = jnp.dot(normed_alpha, project_alpha, preferred_element_type=jnp.float32) + jnp.dot(
        normed_beta, project_beta, preferred_element_type=jnp.float32
    )
    mixed = lax.psum_scatter(term.astype(jnp.bfloat16), "tp", scatter_dimension=1, tiled=True)
    columns = residual_in.shape[1] * heads_tp
    first = depth_scale * residual_in.astype(jnp.float32) + mixed.astype(jnp.float32)
    sums_one = lax.psum((jnp.sum(first, axis=1), jnp.sum(first * first, axis=1)), "tp")
    settled = finish_norm(first, sums_one, gain_settle, bias_settle, columns)
    cap = 3 * rows // count
    flat_ids = expert_ids.reshape(2 * rows)
    onehot = (flat_ids[:, None] == jnp.arange(count, dtype=jnp.int32)[None, :]).astype(jnp.int32)
    before = jnp.cumsum(onehot, axis=0, dtype=jnp.int32) - onehot
    slot = jnp.sum(before * onehot, axis=1, dtype=jnp.int32)
    place = flat_ids * cap + slot
    hit = place[None, :] == jnp.arange(count * cap, dtype=jnp.int32)[:, None]
    owner = jnp.arange(2 * rows, dtype=jnp.int32) // 2
    source = jnp.sum(jnp.where(hit, owner[None, :], 0), axis=1, dtype=jnp.int32)
    filled = jnp.any(hit, axis=1)
    gate_local = expert_gate[0]
    up_local = expert_up[0]
    send = jnp.where(filled[:, None], settled[source], jnp.zeros((), jnp.bfloat16)).reshape(
        count, cap, -1
    )
    arrived = lax.all_to_all(send, "sp", split_axis=0, concat_axis=0, tiled=True)
    piece = lax.all_gather(arrived, "tp", axis=2, tiled=True)
    flat = piece.reshape(-1, piece.shape[2])
    gate = jnp.dot(flat, gate_local, preferred_element_type=jnp.float32)
    up = jnp.dot(flat, up_local, preferred_element_type=jnp.float32)
    hidden = (jax.nn.silu(gate) * up).astype(jnp.bfloat16)
    partial_value = jnp.dot(hidden, expert_down[0], preferred_element_type=jnp.float32).reshape(
        count, cap, -1
    )
    summed = lax.psum_scatter(
        partial_value.astype(jnp.bfloat16), "tp", scatter_dimension=2, tiled=True
    )
    back = lax.all_to_all(summed, "sp", split_axis=0, concat_axis=0, tiled=True).reshape(
        count * cap, -1
    )
    picked = back[place].reshape(rows, 2, -1).astype(jnp.float32)
    routed = route_weight[:, 0:1] * picked[:, 0] + route_weight[:, 1:2] * picked[:, 1]
    second = depth_scale * settled.astype(jnp.float32) + routed
    sums_two = lax.psum((jnp.sum(second, axis=1), jnp.sum(second * second, axis=1)), "tp")
    return finish_norm(second, sums_two, gain_final, bias_final, columns)


GROUP_COUNT = 4
LANE = 128
BF = jnp.bfloat16
F32 = jnp.float32
LOG2E = 1.4426950408889634


def dot(a, b, dims=((1,), (0,))):
    return lax.dot_general(a, b, (dims, ((), ())), preferred_element_type=F32)


def thirds(v):
    hi = v.astype(BF).astype(F32)
    mid = (v - hi).astype(BF).astype(F32)
    return hi, mid, v - hi - mid


def iota(shape, dim):
    return lax.broadcasted_iota(jnp.int32, shape, dim)


def call(kernel, outs, args, scratch=(), name=None):
    smem = pl.BlockSpec(memory_space=pltpu.SMEM)
    vmem = pl.BlockSpec(memory_space=pltpu.VMEM)
    return pl.pallas_call(
        kernel,
        out_shape=outs,
        in_specs=[smem] + [vmem] * (len(args) - 1),
        out_specs=[vmem] * len(outs),
        scratch_shapes=list(scratch),
        name=name,
    )(*args)


def shape_of(shape, dtype=BF):
    return jax.ShapeDtypeStruct(shape, dtype)


def route_kernel(cap, place, ids, idst, weight, resid, m_out, n_out, w_out, r0, r1, r2, r3):
    z, y, c = place[0], place[2], place[3]
    rows = ids.shape[0]
    gcol = lax.shift_right_logical(ids[:, 0:1], 1)
    grow = lax.shift_right_logical(idst[0:1, :], 1)
    same = gcol == grow
    first = iota((rows, rows), 0)
    second = iota((rows, rows), 1)
    slot_col = jnp.sum(jnp.where(same & (second < first), 1.0, 0.0), axis=1, keepdims=True)
    slot_row = jnp.sum(jnp.where(same & (first < second), 1.0, 0.0), axis=0, keepdims=True)
    slot_col = slot_col.astype(jnp.int32)
    slot_row = slot_row.astype(jnp.int32)
    turn = 2 * (z & 1)
    chunk = grow ^ turn
    away_y = lax.shift_right_logical(chunk, 1) ^ y
    away_c = (chunk & 1) ^ c
    spot = away_c * (2 * cap) + away_y * cap + slot_row
    m = jnp.where(iota((4 * cap, rows), 0) == spot, 1.0, 0.0).astype(BF)
    m_out[...] = m
    mine = 2 * y + c
    spot_col = (gcol ^ mine) * cap + slot_col
    n_out[...] = jnp.where(iota((rows, 4 * cap), 1) == spot_col, 1.0, 0.0).astype(BF)
    even = (ids[:, 0:1] & 1) == 0
    w_even = jnp.where(even, weight[:, 0:1], weight[:, 1:2])
    w_odd = jnp.where(even, weight[:, 1:2], weight[:, 0:1])
    lane = iota((rows, LANE), 1)
    table = jnp.zeros((rows, LANE), F32)
    for k, part in enumerate(thirds(w_even) + thirds(w_odd)):
        table = jnp.where(lane == k, part, table)
    w_out[...] = dot(m[:cap], table.astype(BF)).astype(BF)
    moved = dot(m, resid[...]).astype(BF)
    for k, ref in enumerate((r0, r1, r2, r3)):
        ref[...] = moved[k * cap : (k + 1) * cap]


def pack_kernel(place, qa, ka, qb, kb, offs, *outs):
    z, x = place[0], place[1]
    rows = qa.shape[0]
    planes = qa.shape[1] // LANE
    same, cross, vals = outs[:planes], outs[planes : 2 * planes], outs[2 * planes :]

    def offset_rows(ref, values):
        parts = []
        for v in values:
            parts += list(thirds(v))
        parts += [jnp.zeros((1, LANE), F32)] * (8 - len(parts))
        block = jnp.concatenate(parts, axis=0).astype(BF)
        ref[pl.ds(rows, 8), 0:LANE] = block
        ref[pl.ds(rows, 8), LANE : 2 * LANE] = block

    def alpha(ref, u):
        at = pl.multiple_of(u * LANE, LANE)
        ref[0:rows, 0:LANE] = qa[:, pl.ds(at, LANE)]
        ref[0:rows, LANE : 2 * LANE] = ka[:, pl.ds(at, LANE)]
        offset_rows(ref, [offs[pl.ds(2 * u, 1), :], offs[pl.ds(2 * u + 1, 1), :]])

    def beta(ref, u):
        at = pl.multiple_of(u * LANE, LANE)
        ref[0:rows, 0:LANE] = qb[:, pl.ds(at, LANE)]
        ref[0:rows, LANE : 2 * LANE] = kb[:, pl.ds(pl.multiple_of(2 * u * LANE, LANE), LANE)]
        offset_rows(ref, [offs[pl.ds(2 * planes + u, 1), :]])

    for d in range(planes):
        u = (z + d) % planes
        vals[d][...] = kb[:, pl.ds(pl.multiple_of(2 * u * LANE + LANE, LANE), LANE)]

    @pl.when(x == 0)
    def _():
        for d in range(planes):
            alpha(same[d], (z + d) % planes)
            beta(cross[d], (z + d) % planes)

    @pl.when(x != 0)
    def _():
        for d in range(planes):
            beta(same[d], (z + d) % planes)
            alpha(cross[d], (z + d) % planes)


def attend_kernel(planes, place, *refs):
    same, cross = refs[:planes], refs[planes : 2 * planes]
    vsame, vcross = refs[2 * planes : 3 * planes], refs[3 * planes : 4 * planes]
    out_same, out_cross = refs[4 * planes : 5 * planes], refs[5 * planes : 6 * planes]
    q_s, k_s, v_s, off_s, acc_s, rest_s, tri_s = refs[6 * planes :]
    z, x = place[0], place[1]
    rows = vsame[0].shape[0]
    total = 2 * planes * rows
    half = LANE // 2
    lane = iota((rows, LANE), 1)
    low = lane < half

    for d in range(planes):
        for ref, vref, other in ((same[d], vsame[d], x), (cross[d], vcross[d], 1 - x)):
            b = 2 * ((z + planes - d) % planes) + other
            at = pl.ds(pl.multiple_of(b * rows, rows), rows)
            q = ref[0:rows, 0:LANE]
            kv = ref[0:rows, LANE : 2 * LANE]
            lines = ref[pl.ds(rows, 8), 0:LANE].astype(F32)
            for h in range(2):
                off_s[h : h + 1, at] = LOG2E * jnp.sum(lines[3 * h : 3 * h + 3], axis=0, keepdims=True)

            @pl.when(x == 0)
            def _():
                zero = jnp.zeros_like(q)
                q_s[0, at, :] = jnp.where(low, q, zero)
                q_s[1, at, :] = jnp.where(low, zero, q)
                turned = jnp.concatenate([kv[:, half:], kv[:, :half]], axis=1)
                k_s[at, :] = jnp.where(low, kv, turned)
                v_s[at, :] = jnp.where(low, turned, kv)

            @pl.when(x != 0)
            def _():
                q_s[0, at, :] = q
                k_s[at, :] = kv
                v_s[at, :] = vref[...]

    tile = 2 * rows
    tiles = total // tile
    ti = iota((tile, tile), 0)
    tj = iota((tile, tile), 1)
    tri_s[...] = jnp.where(ti >= tj, 1.0, 0.0).astype(BF)
    valid = tj < ti
    scale = jnp.where(x == 0, half ** (-0.5) * LOG2E, LANE ** (-0.5) * LOG2E).astype(F32)

    def one_head(h, carry):
        for i in range(tiles):
            q = q_s[h, i * tile : (i + 1) * tile, :]
            rest = None
            acc = None
            for j in range(i, -1, -1):
                cols = slice(j * tile, (j + 1) * tile)
                s = dot(q, k_s[cols, :], ((1,), (1,))) * scale + off_s[pl.ds(h, 1), cols]
                soft = jnp.maximum(s, 0.0) + jnp.log2(1.0 + jnp.exp2(-jnp.abs(s)))
                if i == j:
                    soft = jnp.where(valid, soft, 0.0)
                hi = soft.astype(BF)
                lo = (soft - hi.astype(F32)).astype(BF)
                cum = dot(hi, tri_s[...]) + dot(lo, tri_s[...])
                if rest is None:
                    w = jnp.exp2(s - cum)
                else:
                    w = jnp.exp2(s - (cum + rest))
                if i == j:
                    w = jnp.where(valid, w, 0.0)
                part = dot(w.astype(BF), v_s[cols, :])
                acc = part if acc is None else acc + part
                if j > 0:
                    rest = cum[:, 0:1] if rest is None else rest + cum[:, 0:1]
            acc_s[h, i * tile : (i + 1) * tile, :] = acc
        return carry

    lax.fori_loop(0, jnp.where(x == 0, 2, 1), one_head, 0)
    for d in range(planes):
        for ref, other in ((out_same[d], x), (out_cross[d], 1 - x)):
            b = 2 * ((z + d) % planes) + other
            at = pl.ds(pl.multiple_of(b * rows, rows), rows)
            one = acc_s[0, at, :]
            ref[...] = jnp.where(low | (x != 0), one, acc_s[1, at, :]).astype(BF)


def collect_kernel(planes, place, *refs):
    same, cross = refs[:planes], refs[planes : 2 * planes]
    gains, out, sums = refs[2 * planes :]
    z, x = place[0], place[1]
    width = planes * LANE
    lane = LANE
    for d in range(planes):
        u = (z + planes - d) % planes
        for ref, kind in ((same[d], x), (cross[d], 1 - x)):
            out[:, pl.ds(pl.multiple_of(kind * width + u * lane, lane), lane)] = ref[...]
    ones = jnp.ones((8, width), F32)
    whole = out[...].astype(F32)
    for k in range(2):
        part = whole[:, k * width : (k + 1) * width]
        line = lax.dot_general(
            ones,
            part * part,
            (((1,), (1,)), ((), ())),
            precision=lax.Precision.HIGHEST,
            preferred_element_type=F32,
        )
        sums[k : k + 1, :] = line[0:1]
    sums[2:8, :] = jnp.zeros((6, sums.shape[1]), F32)
    out[...] = (whole * gains[0:1, :]).astype(BF)


def project_kernel(columns, att, m, s0, s1, s2, s3, pa, pb, keep, send, g_s, f_s):
    half = att.shape[1] // 2

    @pl.when(pl.program_id(0) == 0)
    def _():
        g_s[...] = dot(m[...], att[...]).astype(BF)
        total = s0[0:2, :] + s1[0:2, :] + s2[0:2, :] + s3[0:2, :]
        factor = lax.rsqrt(total / columns + norm_eps)
        mf = m[...].astype(F32)
        for k in range(2):
            f_s[k, :, :] = jnp.sum(mf * factor[k : k + 1], axis=1, keepdims=True)

    a = dot(g_s[:, :half], pa[...]) * f_s[0]
    b = dot(g_s[:, half:], pb[...]) * f_s[1]
    term = (a + b).astype(BF)
    mid = term.shape[0] // 2
    keep[...] = term[:mid]
    send[...] = term[mid:]


def settle_kernel(place, own, got, w, *refs):
    pieces, lines = refs[:4], refs[4:8]
    out, all_lines, res_s = refs[8:]
    t = 2 * place[2] + place[3]
    width = pieces[0].shape[1]
    for k in range(4):
        at = pl.ds(pl.multiple_of((t ^ (2 * (k & 1) + (k >> 1))) * width, LANE), width)
        res_s[:, at] = pieces[k][...]
        all_lines[:, at] = lines[k][...]
    columns = res_s.shape[1]
    mixed = (own[...].astype(F32) + got[...].astype(F32)).astype(BF).astype(F32)
    first = depth_scale * res_s[...].astype(F32) + mixed
    out[:, 0:columns] = row_norm(first, all_lines[0:1, :], all_lines[1:2, :])
    out[:, columns : columns + LANE] = w[...]


def row_norm(total, gain, bias):
    columns = total.shape[1]
    mean = jnp.sum(total, axis=1, keepdims=True) / columns
    var = jnp.sum(total * total, axis=1, keepdims=True) / columns - mean * mean
    return ((total - mean) * lax.rsqrt(var + norm_eps) * gain + bias).astype(BF)


def expert_kernel(place, *refs):
    pieces = refs[:8]
    gate, up, down, near, far, x_s, acc_s, w_s = refs[8:]
    step = pl.program_id(0)
    n = pieces[0].shape[0]
    columns = x_s.shape[1]

    @pl.when(step == 0)
    def _():
        odd = place[1] != 0
        for k in range(8):
            at = slice(k * n, (k + 1) * n)
            x_s[at, :] = pieces[k][:, 0:columns]
            w = pieces[k][:, columns : columns + LANE].astype(F32)
            even_w = w[:, 0:1] + w[:, 1:2] + w[:, 2:3]
            odd_w = w[:, 3:4] + w[:, 4:5] + w[:, 5:6]
            w_s[at, :] = jnp.where(odd, odd_w, even_w)
        acc_s[...] = jnp.zeros_like(acc_s)

    x = x_s[...]
    g = dot(x, gate[0])
    u = dot(x, up[0])
    hidden = (g / (1.0 + jnp.exp(-g)) * u).astype(BF)
    acc_s[...] += dot(hidden, down[0])

    @pl.when(step == pl.num_programs(0) - 1)
    def _():
        mid = 4 * n
        near[...] = (acc_s[0:mid, :] * w_s[0:mid, :]).astype(BF)
        far[...] = (acc_s[mid:, :] * w_s[mid:, :]).astype(BF)


def chip_kernel(near, got, o0, o1, o2, o3):
    n = o0.shape[0]
    total = (near[...].astype(F32) + got[...].astype(F32)).astype(BF)
    for k, ref in enumerate((o0, o1, o2, o3)):
        ref[...] = total[k * n : (k + 1) * n]


def finish_kernel(place, settled, lines, t0, t1, t2, t3, f0, f1, f2, f3, all_s):
    columns = all_s.shape[1]
    routed = t0[...].astype(F32) + t1[...].astype(F32) + t2[...].astype(F32) + t3[...].astype(F32)
    second = depth_scale * settled[:, 0:columns].astype(F32) + routed
    all_s[...] = row_norm(second, lines[2:3, :], lines[3:4, :])
    width = f0.shape[1]
    for k, ref in enumerate((f0, f1, f2, f3)):
        at = pl.ds(pl.multiple_of((place[0] ^ k) * width, LANE), width)
        ref[...] = all_s[:, at]


def place_kernel(n, f0, f1, f2, f3, out):
    cap = f0.shape[0]
    total = dot(n[...], jnp.concatenate([f0[...], f1[...], f2[...], f3[...]], axis=0))
    out[...] = total.astype(BF)


def fast_body(
    chips,
    lanes,
    residual_in,
    query_alpha,
    pairs_alpha,
    offset_alpha,
    gain_alpha,
    query_beta,
    pairs_beta,
    offset_beta,
    gain_beta,
    project_alpha,
    project_beta,
    gain_settle,
    bias_settle,
    expert_ids,
    route_weight,
    expert_gate,
    expert_up,
    expert_down,
    gain_final,
    bias_final,
):
    rows, width = residual_in.shape
    planes = chips // 2
    columns = width * lanes
    cap = 3 * rows // chips
    sp = lax.axis_index("sp")
    tp = lax.axis_index("tp")
    place = jnp.stack([sp // 2, sp % 2, tp // 2, tp % 2]).astype(jnp.int32)
    units = pairs_alpha.shape[1]

    def move(v, dest):
        perm = []
        for a in range(chips * lanes):
            s, t = divmod(a, lanes)
            to = dest(s // 2, s % 2, t)
            if to is not None:
                perm.append((a, (to[0] * 2 + to[1]) * lanes + to[2]))
        return lax.ppermute(v, ("sp", "tp"), perm)

    def shift(v, d, flip):
        return move(v, lambda z, x, t: ((z + d) % planes, x ^ flip, t))

    def swap_tp(v, k):
        return move(v, lambda z, x, t: (z, x, t ^ k))

    def swap_plane(v, dx, k):
        return move(v, lambda z, x, t: (z, x ^ dx, t ^ k))

    def values_to_odd(v, d, flip):
        return move(v, lambda z, x, t: ((z + d) % planes, 1, t) if x ^ flip == 1 else None)

    offs = jnp.concatenate(
        [jnp.transpose(offset_alpha), jnp.transpose(offset_beta), jnp.zeros((units, rows), F32)]
    )
    packed = call(
        pack_kernel,
        [shape_of((rows + 8, 2 * LANE))] * (2 * planes) + [shape_of((rows, LANE))] * planes,
        (
            place,
            query_alpha,
            pairs_alpha.reshape(rows, -1),
            query_beta,
            pairs_beta.reshape(rows, -1),
            offs,
        ),
        name="pack",
    )
    same, cross, vals = packed[:planes], packed[planes : 2 * planes], packed[2 * planes :]
    got_same = [same[0]] + [shift(same[d], d, 0) for d in range(1, planes)]
    got_cross = [shift(cross[d], d, 1) for d in range(planes)]
    got_vsame = [vals[0]] + [values_to_odd(vals[d], d, 0) for d in range(1, planes)]
    got_vcross = [values_to_odd(vals[d], d, 1) for d in range(planes)]

    m, n, w, *res = call(
        lambda *refs: route_kernel(cap, *refs),
        [
            shape_of((4 * cap, rows)),
            shape_of((rows, 4 * cap)),
            shape_of((cap, LANE)),
        ]
        + [shape_of((cap, width))] * 4,
        (place, expert_ids, jnp.transpose(expert_ids), route_weight, residual_in),
        name="route",
    )
    offsets_tp = (0, 2, 1, 3)
    res = [res[0]] + [swap_tp(res[k], offsets_tp[k]) for k in range(1, 4)]
    own_lines = jnp.stack([gain_settle, bias_settle, gain_final, bias_final])
    lines = [own_lines] + [swap_tp(own_lines, offsets_tp[k]) for k in range(1, 4)]

    total = chips * rows
    results = call(
        lambda *refs: attend_kernel(planes, *refs),
        [shape_of((rows, LANE))] * (2 * planes),
        (place, *got_same, *got_cross, *got_vsame, *got_vcross),
        scratch=[
            pltpu.VMEM((2, total, LANE), BF),
            pltpu.VMEM((total, LANE), BF),
            pltpu.VMEM((total, LANE), BF),
            pltpu.VMEM((8, total), F32),
            pltpu.VMEM((2, total, LANE), F32),
            pltpu.VMEM((8, LANE), F32),
            pltpu.VMEM((2 * rows, 2 * rows), BF),
        ],
        name="attend",
    )
    back_same = [results[0]] + [shift(results[d], d, 0) for d in range(1, planes)]
    back_cross = [shift(results[planes + d], d, 1) for d in range(planes)]
    gains = jnp.concatenate([gain_alpha, gain_beta])[None, :]
    att, sums = call(
        lambda *refs: collect_kernel(planes, *refs),
        [shape_of((rows, 2 * width)), shape_of((8, rows), F32)],
        (place, *back_same, *back_cross, gains),
        name="collect",
    )
    all_sums = [sums] + [swap_tp(sums, k) for k in range(1, 4)]

    step = width
    full = lambda shape: pl.BlockSpec(shape, lambda i: (0,) * len(shape))
    by_column = lambda r: pl.BlockSpec((r, step), lambda i: (0, i))
    keep, send = pl.pallas_call(
        lambda *refs: project_kernel(columns, *refs),
        grid=(columns // step,),
        out_shape=[shape_of((2 * cap, columns))] * 2,
        in_specs=[full(att.shape), full(m.shape)]
        + [full(sums.shape)] * 4
        + [by_column(width), by_column(width)],
        out_specs=[by_column(2 * cap)] * 2,
        scratch_shapes=[pltpu.VMEM((4 * cap, 2 * width), BF), pltpu.VMEM((2, 4 * cap, 1), F32)],
        name="project",
    )(att, m, *all_sums, project_alpha, project_beta)
    both = keep.astype(F32) + swap_tp(send, 1).astype(F32)
    got = swap_tp(both[cap:].astype(BF), 2)
    settled, all_lines = call(
        settle_kernel,
        [shape_of((cap, columns + LANE)), shape_of((4, columns), F32)],
        (place, both[:cap].astype(BF), got, w, *res, *lines),
        scratch=[pltpu.VMEM((cap, columns), BF)],
        name="settle",
    )

    def to_plane(z, x, t):
        g = t ^ (2 * (z & 1))
        return g, x, 2 * (t >> 1) + (z >> 1)

    def from_plane(k):
        def dest(g, x, t):
            z = 2 * (t & 1) + ((t >> 1) ^ (g >> 1))
            return z, x, g ^ k

        return dest

    mine = move(settled, to_plane)
    near = [mine, swap_plane(mine, 1, 0), swap_plane(mine, 0, 2), swap_plane(mine, 1, 2)]
    far = [swap_plane(v, 0, 1) for v in near]
    hidden = expert_gate.shape[2]
    chunk = hidden // 4
    settled_spec = pl.BlockSpec((cap, columns + LANE), lambda j: (0, 0))
    half_spec = pl.BlockSpec((4 * cap, columns), lambda j: (0, 0))
    out_near, out_far = pl.pallas_call(
        expert_kernel,
        grid=(hidden // chunk,),
        out_shape=[shape_of((4 * cap, columns))] * 2,
        in_specs=[pl.BlockSpec(memory_space=pltpu.SMEM)]
        + [settled_spec] * 8
        + [
            pl.BlockSpec((1, columns, chunk), lambda j: (0, 0, j)),
            pl.BlockSpec((1, columns, chunk), lambda j: (0, 0, j)),
            pl.BlockSpec((1, chunk, columns), lambda j: (0, j, 0)),
        ],
        out_specs=[half_spec] * 2,
        scratch_shapes=[
            pltpu.VMEM((8 * cap, columns), BF),
            pltpu.VMEM((8 * cap, columns), F32),
            pltpu.VMEM((8 * cap, 1), F32),
        ],
        name="expert",
    )(place, *near, *far, expert_gate, expert_up, expert_down)
    got = swap_plane(out_far, 0, 1)
    vmem = pl.BlockSpec(memory_space=pltpu.VMEM)
    t0, t1, t2, t3 = pl.pallas_call(
        chip_kernel,
        out_shape=[shape_of((cap, columns))] * 4,
        in_specs=[vmem] * 2,
        out_specs=[vmem] * 4,
        name="chip",
    )(out_near, got)
    t1, t2, t3 = swap_plane(t1, 1, 0), swap_plane(t2, 0, 2), swap_plane(t3, 1, 2)
    ends = call(
        finish_kernel,
        [shape_of((cap, width))] * 4,
        (place, mine, all_lines, t0, t1, t2, t3),
        scratch=[pltpu.VMEM((cap, columns), BF)],
        name="finish",
    )
    home = [move(ends[k], from_plane(k)) for k in range(4)]
    return pl.pallas_call(
        place_kernel,
        out_shape=shape_of((rows, width)),
        in_specs=[vmem] * 5,
        out_specs=vmem,
        name="place",
    )(n, *home)


def solution(mesh):
    chips, lanes = mesh.shape["sp"], mesh.shape["tp"]

    def body(*args):
        residual_in, pairs_alpha, pairs_beta = args[0], args[2], args[6]
        planes = chips // 2
        fast = (
            chips // GROUP_COUNT == 2
            and lanes == planes
            and lanes == 4
            and pairs_alpha.shape[1] == planes
            and pairs_beta.shape[1] == planes
            and pairs_alpha.shape[2] == LANE
            and pairs_beta.shape[2] == 2 * LANE
            and residual_in.shape[0] == LANE
            and args[1].shape[1] == planes * LANE
            and args[5].shape[1] == planes * LANE
        )
        return fast_body(chips, lanes, *args) if fast else general_body(*args)

    in_specs = (
        P("sp", "tp"),
        P("sp", "tp"),
        P("sp", "tp", None),
        P("sp", "tp"),
        P("tp"),
        P("sp", "tp"),
        P("sp", "tp", None),
        P("sp", "tp"),
        P("tp"),
        P("tp", None),
        P("tp", None),
        P("tp"),
        P("tp"),
        P("sp", None),
        P("sp", None),
        P("sp", None, "tp"),
        P("sp", None, "tp"),
        P("sp", "tp", None),
        P("tp"),
        P("tp"),
    )
    out_specs = P("sp", "tp")
    return jax.shard_map(body, mesh=mesh, in_specs=in_specs, out_specs=out_specs, check_vma=False)
```

```python
import jax
import jax.numpy as jnp
from jax import lax
from jax.experimental import pallas as pl
from jax.experimental.pallas import tpu as pltpu
from jax.sharding import PartitionSpec as P

depth_scale = 2.0**0.5
norm_eps = 1e-05


def break_block(acc, remain, queries, pairs, offsets, key_first, query_first):
    width = queries.shape[3]
    keys = pairs[:, :, :width]
    values = pairs[:, :, width:]
    length = offsets.shape[0]
    kv_heads = queries.shape[1]
    share = queries.shape[2]
    scores = jnp.einsum(
        "qhrd,khd->hrqk", queries, keys, preferred_element_type=jnp.float32
    ) * width ** (-0.5)
    scores = (
        scores + jnp.transpose(offsets.reshape(length, kv_heads, share), (1, 2, 0))[:, :, None, :]
    )
    query_pos = query_first + jnp.arange(queries.shape[0], dtype=jnp.int32)
    key_pos = key_first + jnp.arange(length, dtype=jnp.int32)
    valid = key_pos[None, :] < query_pos[:, None]
    soft = jnp.where(valid, jax.nn.softplus(scores), 0.0)
    later = lax.cumsum(soft, axis=3, reverse=True) - soft
    weights = jnp.where(
        valid, jnp.exp(jax.nn.log_sigmoid(scores) - later + remain[..., None]), 0.0
    ).astype(jnp.bfloat16)
    acc = acc + jnp.einsum("hrqk,khd->qhrd", weights, values, preferred_element_type=jnp.float32)
    return (acc, remain - jnp.sum(soft, axis=3))


def finish_norm(total, sums, gain, bias, columns):
    mean = sums[0] / columns
    var = sums[1] / columns - mean * mean
    return ((total - mean[:, None]) * lax.rsqrt(var + norm_eps)[:, None] * gain + bias).astype(
        jnp.bfloat16
    )


def general_body(
    residual_in,
    query_alpha,
    pairs_alpha,
    offset_alpha,
    gain_alpha,
    query_beta,
    pairs_beta,
    offset_beta,
    gain_beta,
    project_alpha,
    project_beta,
    gain_settle,
    bias_settle,
    expert_ids,
    route_weight,
    expert_gate,
    expert_up,
    expert_down,
    gain_final,
    bias_final,
):
    rows = residual_in.shape[0]
    mine = lax.axis_index("sp")
    count = lax.axis_size("sp")
    heads_tp = lax.axis_size("tp")
    width_alpha = pairs_alpha.shape[2] // 2
    width_beta = pairs_beta.shape[2] // 2
    grouped_alpha = query_alpha.reshape(rows, pairs_alpha.shape[1], -1, width_alpha)
    grouped_beta = query_beta.reshape(rows, pairs_beta.shape[1], -1, width_beta)
    query_first = mine * rows
    initial = (
        jnp.zeros(grouped_alpha.shape, jnp.float32),
        jnp.zeros(grouped_beta.shape, jnp.float32),
        jnp.zeros((grouped_alpha.shape[1], grouped_alpha.shape[2], rows), jnp.float32),
        jnp.zeros((grouped_beta.shape[1], grouped_beta.shape[2], rows), jnp.float32),
    )

    def visit(state, pairs, offsets, key_first):
        acc_alpha, acc_beta, rest_alpha, rest_beta = state
        acc_alpha, rest_alpha = break_block(
            acc_alpha, rest_alpha, grouped_alpha, pairs[0], offsets[0], key_first, query_first
        )
        acc_beta, rest_beta = break_block(
            acc_beta, rest_beta, grouped_beta, pairs[1], offsets[1], key_first, query_first
        )
        return (acc_alpha, acc_beta, rest_alpha, rest_beta)

    def maybe_visit(state, turn, pairs, offsets):
        return lax.cond(
            turn <= mine,
            lambda kept: visit(kept, pairs, offsets, (mine - turn) * rows),
            lambda kept: kept,
            state,
        )

    pairs_all = (
        lax.all_gather(pairs_alpha, "sp", axis=0, tiled=True),
        lax.all_gather(pairs_beta, "sp", axis=0, tiled=True),
    )
    offsets_all = (
        lax.all_gather(offset_alpha, "sp", axis=0, tiled=True),
        lax.all_gather(offset_beta, "sp", axis=0, tiled=True),
    )

    def turn_all(turn, state):
        first_row = (mine - turn) * rows
        pairs = (
            lax.dynamic_slice_in_dim(pairs_all[0], first_row, rows, 0),
            lax.dynamic_slice_in_dim(pairs_all[1], first_row, rows, 0),
        )
        offsets = (
            lax.dynamic_slice_in_dim(offsets_all[0], first_row, rows, 0),
            lax.dynamic_slice_in_dim(offsets_all[1], first_row, rows, 0),
        )
        return maybe_visit(state, turn, pairs, offsets)

    state = lax.fori_loop(0, count, turn_all, initial)
    attend_alpha = state[0].reshape(rows, -1)
    attend_beta = state[1].reshape(rows, -1)
    squares = lax.psum(
        (jnp.sum(attend_alpha * attend_alpha, axis=1), jnp.sum(attend_beta * attend_beta, axis=1)),
        "tp",
    )
    scale_alpha = lax.rsqrt(squares[0] / (attend_alpha.shape[1] * heads_tp) + norm_eps)
    scale_beta = lax.rsqrt(squares[1] / (attend_beta.shape[1] * heads_tp) + norm_eps)
    normed_alpha = (attend_alpha * scale_alpha[:, None] * gain_alpha).astype(jnp.bfloat16)
    normed_beta = (attend_beta * scale_beta[:, None] * gain_beta).astype(jnp.bfloat16)
    term = jnp.dot(normed_alpha, project_alpha, preferred_element_type=jnp.float32) + jnp.dot(
        normed_beta, project_beta, preferred_element_type=jnp.float32
    )
    mixed = lax.psum_scatter(term.astype(jnp.bfloat16), "tp", scatter_dimension=1, tiled=True)
    columns = residual_in.shape[1] * heads_tp
    first = depth_scale * residual_in.astype(jnp.float32) + mixed.astype(jnp.float32)
    sums_one = lax.psum((jnp.sum(first, axis=1), jnp.sum(first * first, axis=1)), "tp")
    settled = finish_norm(first, sums_one, gain_settle, bias_settle, columns)
    cap = 3 * rows // count
    flat_ids = expert_ids.reshape(2 * rows)
    onehot = (flat_ids[:, None] == jnp.arange(count, dtype=jnp.int32)[None, :]).astype(jnp.int32)
    before = jnp.cumsum(onehot, axis=0, dtype=jnp.int32) - onehot
    slot = jnp.sum(before * onehot, axis=1, dtype=jnp.int32)
    place = flat_ids * cap + slot
    hit = place[None, :] == jnp.arange(count * cap, dtype=jnp.int32)[:, None]
    owner = jnp.arange(2 * rows, dtype=jnp.int32) // 2
    source = jnp.sum(jnp.where(hit, owner[None, :], 0), axis=1, dtype=jnp.int32)
    filled = jnp.any(hit, axis=1)
    gate_local = expert_gate[0]
    up_local = expert_up[0]
    send = jnp.where(filled[:, None], settled[source], jnp.zeros((), jnp.bfloat16)).reshape(
        count, cap, -1
    )
    arrived = lax.all_to_all(send, "sp", split_axis=0, concat_axis=0, tiled=True)
    piece = lax.all_gather(arrived, "tp", axis=2, tiled=True)
    flat = piece.reshape(-1, piece.shape[2])
    gate = jnp.dot(flat, gate_local, preferred_element_type=jnp.float32)
    up = jnp.dot(flat, up_local, preferred_element_type=jnp.float32)
    hidden = (jax.nn.silu(gate) * up).astype(jnp.bfloat16)
    partial_value = jnp.dot(hidden, expert_down[0], preferred_element_type=jnp.float32).reshape(
        count, cap, -1
    )
    summed = lax.psum_scatter(
        partial_value.astype(jnp.bfloat16), "tp", scatter_dimension=2, tiled=True
    )
    back = lax.all_to_all(summed, "sp", split_axis=0, concat_axis=0, tiled=True).reshape(
        count * cap, -1
    )
    picked = back[place].reshape(rows, 2, -1).astype(jnp.float32)
    routed = route_weight[:, 0:1] * picked[:, 0] + route_weight[:, 1:2] * picked[:, 1]
    second = depth_scale * settled.astype(jnp.float32) + routed
    sums_two = lax.psum((jnp.sum(second, axis=1), jnp.sum(second * second, axis=1)), "tp")
    return finish_norm(second, sums_two, gain_final, bias_final, columns)


GROUP_COUNT = 4
LANE = 128
BF = jnp.bfloat16
F32 = jnp.float32
LOG2E = 1.4426950408889634


def dot(a, b, dims=((1,), (0,))):
    return lax.dot_general(a, b, (dims, ((), ())), preferred_element_type=F32)


def thirds(v):
    hi = v.astype(BF).astype(F32)
    mid = (v - hi).astype(BF).astype(F32)
    return hi, mid, v - hi - mid


def iota(shape, dim):
    return lax.broadcasted_iota(jnp.int32, shape, dim)


def call(kernel, outs, args, vmem, scratch=(), hidden=0, name=None):
    local = pl.BlockSpec(memory_space=pltpu.VMEM)
    spare = pl.BlockSpec(memory_space=pl.ANY)
    return pl.pallas_call(
        kernel,
        out_shape=outs,
        in_specs=[local] * (len(args) - hidden) + [spare] * hidden,
        out_specs=[local] * len(outs),
        scratch_shapes=list(scratch),
        compiler_params=pltpu.CompilerParams(vmem_limit_bytes=vmem << 20),
        name=name,
    )(*args)


def spot():
    sp = lax.axis_index("sp")
    tp = lax.axis_index("tp")
    return sp // 2, sp % 2, tp


def in_hbm(*values):
    return tuple(pltpu.with_memory_space_constraint(v, pltpu.HBM) for v in values)


def shape_of(shape, dtype=BF):
    return jax.ShapeDtypeStruct(shape, dtype)


def route_kernel(cap, ids, weight, *refs):
    m_out, n_out, w_out = refs[-3:]
    z, _, t = spot()
    rows = ids.shape[1]
    first = iota((rows, rows), 0)
    second = iota((rows, rows), 1)

    def column(line):
        return jnp.sum(jnp.where(first == second, line, 0), axis=1, keepdims=True)

    grow = lax.shift_right_logical(ids[0:1, :], 1)
    gcol = column(grow)
    same = gcol == grow
    slot_col = jnp.sum(jnp.where(same & (second < first), 1, 0), axis=1, keepdims=True)
    slot_row = jnp.sum(jnp.where(same & (first < second), 1, 0), axis=0, keepdims=True)
    away = (grow ^ (2 * (z & 1))) ^ t
    block = 2 * (away & 1) + lax.shift_right_logical(away, 1)
    m = jnp.where(iota((4 * cap, rows), 0) == block * cap + slot_row, 1.0, 0.0).astype(BF)
    m_out[...] = m
    place = (gcol ^ t) * cap + slot_col
    n_out[...] = jnp.where(iota((rows, 4 * cap), 1) == place, 1.0, 0.0).astype(BF)
    even = (ids[0:1, :] & 1) == 0
    w_even = column(jnp.where(even, weight[0:1, :], weight[1:2, :]))
    w_odd = column(jnp.where(even, weight[1:2, :], weight[0:1, :]))
    lane = iota((rows, LANE), 1)
    table = jnp.zeros((rows, LANE), F32)
    for k, part in enumerate(thirds(w_even) + thirds(w_odd)):
        table = jnp.where(lane == k, part, table)
    w_out[...] = dot(m[:cap], table.astype(BF)).astype(BF)


def pack_kernel(qa, ka, qb, kb, offs_a, offs_b, *outs):
    z, x, _ = spot()
    rows = qa.shape[0]
    planes = qa.shape[1] // LANE
    half = LANE // 2
    sides = (outs[:planes], outs[planes : 2 * planes])
    low = iota((rows, LANE), 1) < half

    def offset_rows(ref, values):
        parts = []
        for v in values:
            parts += list(thirds(v))
        parts += [jnp.zeros((1, LANE), F32)] * (8 - len(parts))
        block = jnp.concatenate(parts, axis=0).astype(BF)
        for k in range(3):
            ref[pl.ds(rows, 8), k * LANE : (k + 1) * LANE] = block

    all_a = ka[...].astype(F32)
    all_b = kb[...].astype(F32)
    for u in range(planes):
        d = (u + planes - z) % planes
        cols = slice(u * LANE, (u + 1) * LANE)
        kv = all_a[:, u, :].astype(BF)
        kv_beta = all_b[:, u, :].astype(BF)
        turned = jnp.concatenate([kv[:, half:], kv[:, :half]], axis=1)
        for k in range(planes):

            @pl.when(d == k)
            def _():
                for flip in range(2):

                    @pl.when(x == flip)
                    def _():
                        alpha, beta = sides[flip][k], sides[1 - flip][k]
                        alpha[0:rows, 0:LANE] = qa[:, cols]
                        alpha[0:rows, LANE : 2 * LANE] = jnp.where(low, kv, turned)
                        alpha[0:rows, 2 * LANE :] = jnp.where(low, turned, kv)
                        offset_rows(alpha, [offs_a[2 * u : 2 * u + 1, :], offs_a[2 * u + 1 : 2 * u + 2, :]])
                        beta[0:rows, 0:LANE] = qb[:, cols]
                        beta[0:rows, LANE:] = kv_beta
                        offset_rows(beta, [offs_b[u : u + 1, :]])


def attend_kernel(planes, spare, *refs):
    same, cross = refs[:planes], refs[planes : 2 * planes]
    refs = refs[2 * planes + spare :]
    out_same, out_cross = refs[:planes], refs[planes : 2 * planes]
    q_s, k_s, v_s, off_s, acc_s, tri_s = refs[2 * planes :]
    z, x, _ = spot()
    rows = out_same[0].shape[0]
    total = 2 * planes * rows
    half = LANE // 2
    low = iota((rows, LANE), 1) < half

    for d in range(planes):
        for ref, other in ((same[d], x), (cross[d], 1 - x)):
            b = 2 * ((z + planes - d) % planes) + other
            at = pl.ds(pl.multiple_of(b * rows, rows), rows)
            q = ref[0:rows, 0:LANE]
            zero = jnp.zeros_like(q)
            q_s[0, at, :] = jnp.where(low | (x != 0), q, zero)
            q_s[1, at, :] = jnp.where(low, zero, q)
            k_s[at, :] = ref[0:rows, LANE : 2 * LANE]
            v_s[at, :] = ref[0:rows, 2 * LANE :]
            lines = ref[pl.ds(rows, 8), 0:LANE].astype(F32)
            for h in range(2):
                off_s[h : h + 1, at] = LOG2E * jnp.sum(lines[3 * h : 3 * h + 3], axis=0, keepdims=True)

    tile = 2 * rows
    tiles = total // tile
    ti = iota((tile, tile), 0)
    tj = iota((tile, tile), 1)
    tri_s[...] = jnp.where(ti >= tj, 1.0, 0.0).astype(BF)
    valid = tj < ti
    scale = jnp.where(x == 0, half ** (-0.5) * LOG2E, LANE ** (-0.5) * LOG2E).astype(F32)

    def one_head(h, carry):
        for i in range(tiles):
            q = q_s[h, i * tile : (i + 1) * tile, :]
            rest = None
            acc = None
            for j in range(i, -1, -1):
                cols = slice(j * tile, (j + 1) * tile)
                s = dot(q, k_s[cols, :], ((1,), (1,))) * scale + off_s[pl.ds(h, 1), cols]
                soft = jnp.maximum(s, 0.0) + jnp.log2(1.0 + jnp.exp2(-jnp.abs(s)))
                if i == j:
                    soft = jnp.where(valid, soft, 0.0)
                hi = soft.astype(BF)
                lo = (soft - hi.astype(F32)).astype(BF)
                cum = dot(hi, tri_s[...]) + dot(lo, tri_s[...])
                if rest is None:
                    w = jnp.exp2(s - cum)
                else:
                    w = jnp.exp2(s - (cum + rest))
                if i == j:
                    w = jnp.where(valid, w, 0.0)
                part = dot(w.astype(BF), v_s[cols, :])
                acc = part if acc is None else acc + part
                if j > 0:
                    rest = cum[:, 0:1] if rest is None else rest + cum[:, 0:1]
            acc_s[h, i * tile : (i + 1) * tile, :] = acc
        return carry

    lax.fori_loop(0, jnp.where(x == 0, 2, 1), one_head, 0)
    for d in range(planes):
        for ref, other in ((out_same[d], x), (out_cross[d], 1 - x)):
            b = 2 * ((z + d) % planes) + other
            at = pl.ds(pl.multiple_of(b * rows, rows), rows)
            one = acc_s[0, at, :]
            ref[...] = jnp.where(low | (x != 0), one, acc_s[1, at, :]).astype(BF)


def collect_kernel(planes, *refs):
    same, cross = refs[:planes], refs[planes : 2 * planes]
    gains, out, sums = refs[2 * planes :]
    z, x, _ = spot()
    width = planes * LANE
    lane = LANE
    for d in range(planes):
        u = (z + planes - d) % planes
        for ref, kind in ((same[d], x), (cross[d], 1 - x)):
            out[:, pl.ds(pl.multiple_of(kind * width + u * lane, lane), lane)] = ref[...]
    ones = jnp.ones((8, width), F32)
    whole = out[...].astype(F32)
    for k in range(2):
        part = whole[:, k * width : (k + 1) * width]
        line = lax.dot_general(
            ones,
            part * part,
            (((1,), (1,)), ((), ())),
            precision=lax.Precision.HIGHEST,
            preferred_element_type=F32,
        )
        sums[k : k + 1, :] = line[0:1]
    sums[2:8, :] = jnp.zeros((6, sums.shape[1]), F32)
    out[...] = (whole * gains[0:1, :]).astype(BF)


def project_kernel(columns, att, m, resid, s0, s1, s2, s3, pa, pb, keep, send, g_s, f_s):
    half = att.shape[1] // 2

    @pl.when(pl.program_id(0) == 0)
    def _():
        g_s[...] = dot(m[...], att[...]).astype(BF)
        total = s0[0:2, :] + s1[0:2, :] + s2[0:2, :] + s3[0:2, :]
        factor = lax.rsqrt(total / columns + norm_eps)
        mf = m[...].astype(F32)
        for k in range(2):
            f_s[k, :, :] = jnp.sum(mf * factor[k : k + 1], axis=1, keepdims=True)

    a = dot(g_s[:, :half], pa[...]) * f_s[0]
    b = dot(g_s[:, half:], pb[...]) * f_s[1]
    own = pl.program_id(0) == lax.axis_index("tp")
    a = a + jnp.where(own, depth_scale, 0.0) * dot(m[...], resid[...])
    term = (a + b).astype(BF)
    mid = term.shape[0] // 2
    keep[...] = term[:mid]
    send[...] = term[mid:]


def pair_kernel(keep, got, own, send):
    n = own.shape[0]
    total = keep[...].astype(F32) + got[...].astype(F32)
    own[...] = total[:n]
    send[...] = total[n:].astype(BF)


def settle_kernel(own, got, w, l0, l1, l2, l3, out, lines):
    _, _, t = spot()
    width = l0.shape[1]
    for k, ref in enumerate((l0, l1, l2, l3)):
        lines[:, pl.ds(pl.multiple_of((t ^ k) * width, LANE), width)] = ref[...]
    columns = lines.shape[1]
    first = own[...] + got[...].astype(F32)
    out[:, 0:columns] = row_norm(first, lines[0:1, :], lines[1:2, :])
    out[:, columns : columns + LANE] = w[...]


def row_norm(total, gain, bias):
    columns = total.shape[1]
    mean = jnp.sum(total, axis=1, keepdims=True) / columns
    var = jnp.sum(total * total, axis=1, keepdims=True) / columns - mean * mean
    return ((total - mean) * lax.rsqrt(var + norm_eps) * gain + bias).astype(BF)


def expert_kernel(*refs):
    pieces = refs[:8]
    gate, up, down, near, far, x_s, acc_s, w_s = refs[8:]
    step = pl.program_id(0)
    n = pieces[0].shape[0]
    columns = x_s.shape[1]

    @pl.when(step == 0)
    def _():
        odd = lax.axis_index("sp") % 2 != 0
        for k in range(8):
            at = slice(k * n, (k + 1) * n)
            x_s[at, :] = pieces[k][:, 0:columns]
            w = pieces[k][:, columns : columns + LANE].astype(F32)
            even_w = w[:, 0:1] + w[:, 1:2] + w[:, 2:3]
            odd_w = w[:, 3:4] + w[:, 4:5] + w[:, 5:6]
            w_s[at, :] = jnp.where(odd, odd_w, even_w)
        acc_s[...] = jnp.zeros_like(acc_s)

    x = x_s[...]
    g = dot(x, gate[0])
    u = dot(x, up[0])
    hidden = (g / (1.0 + jnp.exp(-g)) * u).astype(BF)
    acc_s[...] += dot(hidden, down[0])

    @pl.when(step == pl.num_programs(0) - 1)
    def _():
        mid = 4 * n
        near[...] = (acc_s[0:mid, :] * w_s[0:mid, :]).astype(BF)
        far[...] = (acc_s[mid:, :] * w_s[mid:, :]).astype(BF)


def chip_kernel(near, got, o0, o1, o2, o3):
    n = o0.shape[0]
    total = (near[...].astype(F32) + got[...].astype(F32)).astype(BF)
    for k, ref in enumerate((o0, o1, o2, o3)):
        ref[...] = total[k * n : (k + 1) * n]


def finish_kernel(settled, lines, t0, t1, t2, t3, f0, f1, f2, f3, all_s):
    columns = all_s.shape[1]
    routed = t0[...].astype(F32) + t1[...].astype(F32) + t2[...].astype(F32) + t3[...].astype(F32)
    second = depth_scale * settled[:, 0:columns].astype(F32) + routed
    all_s[...] = row_norm(second, lines[2:3, :], lines[3:4, :])
    width = f0.shape[1]
    for k, ref in enumerate((f0, f1, f2, f3)):
        at = pl.ds(pl.multiple_of((spot()[0] ^ k) * width, LANE), width)
        ref[...] = all_s[:, at]


def place_kernel(n, f0, f1, f2, f3, out):
    cap = f0.shape[0]
    total = dot(n[...], jnp.concatenate([f0[...], f1[...], f2[...], f3[...]], axis=0))
    out[...] = total.astype(BF)


def fast_body(
    chips,
    lanes,
    residual_in,
    query_alpha,
    pairs_alpha,
    offset_alpha,
    gain_alpha,
    query_beta,
    pairs_beta,
    offset_beta,
    gain_beta,
    project_alpha,
    project_beta,
    gain_settle,
    bias_settle,
    expert_ids,
    route_weight,
    expert_gate,
    expert_up,
    expert_down,
    gain_final,
    bias_final,
):
    rows, width = residual_in.shape
    planes = chips // 2
    columns = width * lanes
    cap = 3 * rows // chips

    def move(v, dest):
        perm = []
        for a in range(chips * lanes):
            s, t = divmod(a, lanes)
            to = dest(s // 2, s % 2, t)
            if to is not None:
                perm.append((a, (to[0] * 2 + to[1]) * lanes + to[2]))
        return lax.ppermute(v, ("sp", "tp"), perm)

    def shift(v, d, flip):
        return move(v, lambda z, x, t: ((z + d) % planes, x ^ flip, t))

    def swap_tp(v, k):
        return move(v, lambda z, x, t: (z, x, t ^ k))

    def swap_plane(v, dx, k):
        return move(v, lambda z, x, t: (z, x ^ dx, t ^ k))

    packed = call(
        pack_kernel,
        [shape_of((rows + 8, 3 * LANE))] * (2 * planes),
        in_hbm(
            query_alpha,
            pairs_alpha,
            query_beta,
            pairs_beta,
            jnp.transpose(offset_alpha),
            jnp.transpose(offset_beta),
        ),
        12,
        name="pack",
    )
    same, cross = packed[:planes], packed[planes:]
    got_same, got_cross = [same[0]] + [None] * (planes - 1), [None] * planes
    for d in (2, 1, 3, 0):
        got_cross[d] = shift(cross[d], d, 1)
        if d:
            got_same[d] = shift(same[d], d, 0)

    m, n, w = call(
        lambda *refs: route_kernel(cap, *refs),
        [shape_of((4 * cap, rows)), shape_of((rows, 4 * cap)), shape_of((cap, LANE))],
        (*in_hbm(jnp.transpose(expert_ids), jnp.transpose(route_weight)), got_cross[2]),
        8,
        hidden=1,
        name="route",
    )
    own_lines = jnp.stack([gain_settle, bias_settle, gain_final, bias_final])
    lines = [own_lines] + [swap_tp(own_lines, k) for k in range(1, 4)]

    total = chips * rows
    spare = (m, n, w, *lines[1:])
    results = call(
        lambda *refs: attend_kernel(planes, len(spare), *refs),
        [shape_of((rows, LANE))] * (2 * planes),
        (*got_same, *got_cross, *spare),
        20,
        hidden=len(spare),
        scratch=[
            pltpu.VMEM((2, total, LANE), BF),
            pltpu.VMEM((total, LANE), BF),
            pltpu.VMEM((total, LANE), BF),
            pltpu.VMEM((8, total), F32),
            pltpu.VMEM((2, total, LANE), F32),
            pltpu.VMEM((2 * rows, 2 * rows), BF),
        ],
        name="attend",
    )
    back_same = [results[0]] + [shift(results[d], d, 0) for d in range(1, planes)]
    back_cross = [shift(results[planes + d], d, 1) for d in range(planes)]
    gains = jnp.concatenate([gain_alpha, gain_beta])[None, :]
    att, sums = call(
        lambda *refs: collect_kernel(planes, *refs),
        [shape_of((rows, 2 * width)), shape_of((8, rows), F32)],
        (*back_same, *back_cross, gains),
        8,
        name="collect",
    )
    all_sums = [sums] + [swap_tp(sums, k) for k in range(1, 4)]

    step = width
    full = lambda shape: pl.BlockSpec(shape, lambda i: (0,) * len(shape))
    by_column = lambda r: pl.BlockSpec((r, step), lambda i: (0, i))
    keep, send = pl.pallas_call(
        lambda *refs: project_kernel(columns, *refs),
        grid=(columns // step,),
        out_shape=[shape_of((2 * cap, columns))] * 2,
        in_specs=[full(att.shape), full(m.shape), full(residual_in.shape)]
        + [full(sums.shape)] * 4
        + [by_column(width), by_column(width)],
        out_specs=[by_column(2 * cap)] * 2,
        scratch_shapes=[pltpu.VMEM((4 * cap, 2 * width), BF), pltpu.VMEM((2, 4 * cap, 1), F32)],
        compiler_params=pltpu.CompilerParams(vmem_limit_bytes=16 << 20),
        name="project",
    )(att, m, *in_hbm(residual_in), *all_sums, *in_hbm(project_alpha, project_beta))
    own, send = call(
        pair_kernel,
        [shape_of((cap, columns), F32), shape_of((cap, columns))],
        (keep, swap_tp(send, 1)),
        8,
        name="pair",
    )
    settled, all_lines = call(
        settle_kernel,
        [shape_of((cap, columns + LANE)), shape_of((4, columns), F32)],
        (own, swap_tp(send, 2), w, *lines),
        8,
        name="settle",
    )

    def to_plane(z, x, t):
        g = t ^ (2 * (z & 1))
        return g, x, 2 * (t >> 1) + (z >> 1)

    def from_plane(k):
        def dest(g, x, t):
            z = 2 * (t & 1) + ((t >> 1) ^ (g >> 1))
            return z, x, g ^ k

        return dest

    mine = move(settled, to_plane)
    near = [mine, swap_plane(mine, 1, 0), swap_plane(mine, 0, 2), swap_plane(mine, 1, 2)]
    far = [swap_plane(v, 0, 1) for v in near]
    hidden = expert_gate.shape[2]
    chunk = hidden // 4
    settled_spec = pl.BlockSpec((cap, columns + LANE), lambda j: (0, 0))
    half_spec = pl.BlockSpec((4 * cap, columns), lambda j: (0, 0))
    out_near, out_far = pl.pallas_call(
        expert_kernel,
        grid=(hidden // chunk,),
        out_shape=[shape_of((4 * cap, columns))] * 2,
        in_specs=[settled_spec] * 8
        + [
            pl.BlockSpec((1, columns, chunk), lambda j: (0, 0, j)),
            pl.BlockSpec((1, columns, chunk), lambda j: (0, 0, j)),
            pl.BlockSpec((1, chunk, columns), lambda j: (0, j, 0)),
        ],
        out_specs=[half_spec] * 2,
        scratch_shapes=[
            pltpu.VMEM((8 * cap, columns), BF),
            pltpu.VMEM((8 * cap, columns), F32),
            pltpu.VMEM((8 * cap, 1), F32),
        ],
        compiler_params=pltpu.CompilerParams(vmem_limit_bytes=28 << 20),
        name="expert",
    )(*near, *far, *in_hbm(expert_gate, expert_up, expert_down))
    got = swap_plane(out_far, 0, 1)
    t0, t1, t2, t3 = call(chip_kernel, [shape_of((cap, columns))] * 4, (out_near, got), 8, name="chip")
    t1, t2, t3 = swap_plane(t1, 1, 0), swap_plane(t2, 0, 2), swap_plane(t3, 1, 2)
    ends = call(
        finish_kernel,
        [shape_of((cap, width))] * 4,
        (mine, all_lines, t0, t1, t2, t3),
        8,
        scratch=[pltpu.VMEM((cap, columns), BF)],
        name="finish",
    )
    home = [move(ends[k], from_plane(k)) for k in range(4)]
    (out,) = call(place_kernel, [shape_of((rows, width))], (n, *home), 4, name="place")
    return out


def solution(mesh):
    chips, lanes = mesh.shape["sp"], mesh.shape["tp"]

    def body(*args):
        residual_in, pairs_alpha, pairs_beta = args[0], args[2], args[6]
        planes = chips // 2
        fast = (
            chips // GROUP_COUNT == 2
            and lanes == planes
            and lanes == 4
            and pairs_alpha.shape[1] == planes
            and pairs_beta.shape[1] == planes
            and pairs_alpha.shape[2] == LANE
            and pairs_beta.shape[2] == 2 * LANE
            and residual_in.shape[0] == LANE
            and args[1].shape[1] == planes * LANE
            and args[5].shape[1] == planes * LANE
        )
        return fast_body(chips, lanes, *args) if fast else general_body(*args)

    in_specs = (
        P("sp", "tp"),
        P("sp", "tp"),
        P("sp", "tp", None),
        P("sp", "tp"),
        P("tp"),
        P("sp", "tp"),
        P("sp", "tp", None),
        P("sp", "tp"),
        P("tp"),
        P("tp", None),
        P("tp", None),
        P("tp"),
        P("tp"),
        P("sp", None),
        P("sp", None),
        P("sp", None, "tp"),
        P("sp", None, "tp"),
        P("sp", "tp", None),
        P("tp"),
        P("tp"),
    )
    out_specs = P("sp", "tp")
    return jax.shard_map(body, mesh=mesh, in_specs=in_specs, out_specs=out_specs, check_vma=False)
```

```python
import jax
import jax.numpy as jnp
from jax import lax
from jax.experimental import pallas as pl
from jax.experimental.pallas import tpu as pltpu
from jax.sharding import PartitionSpec as P


depth_scale = 2.0**0.5
norm_eps = 1e-05


def break_block(acc, remain, queries, pairs, offsets, key_first, query_first):
    width = queries.shape[3]
    keys = pairs[:, :, :width]
    values = pairs[:, :, width:]
    length = offsets.shape[0]
    kv_heads = queries.shape[1]
    share = queries.shape[2]
    scores = jnp.einsum(
        "qhrd,khd->hrqk", queries, keys, preferred_element_type=jnp.float32
    ) * width ** (-0.5)
    scores = (
        scores + jnp.transpose(offsets.reshape(length, kv_heads, share), (1, 2, 0))[:, :, None, :]
    )
    query_pos = query_first + jnp.arange(queries.shape[0], dtype=jnp.int32)
    key_pos = key_first + jnp.arange(length, dtype=jnp.int32)
    valid = key_pos[None, :] < query_pos[:, None]
    soft = jnp.where(valid, jax.nn.softplus(scores), 0.0)
    later = lax.cumsum(soft, axis=3, reverse=True) - soft
    weights = jnp.where(
        valid, jnp.exp(jax.nn.log_sigmoid(scores) - later + remain[..., None]), 0.0
    ).astype(jnp.bfloat16)
    acc = acc + jnp.einsum("hrqk,khd->qhrd", weights, values, preferred_element_type=jnp.float32)
    return (acc, remain - jnp.sum(soft, axis=3))


def finish_norm(total, sums, gain, bias, columns):
    mean = sums[0] / columns
    var = sums[1] / columns - mean * mean
    return ((total - mean[:, None]) * lax.rsqrt(var + norm_eps)[:, None] * gain + bias).astype(
        jnp.bfloat16
    )


def general_body(
    residual_in,
    query_alpha,
    pairs_alpha,
    offset_alpha,
    gain_alpha,
    query_beta,
    pairs_beta,
    offset_beta,
    gain_beta,
    project_alpha,
    project_beta,
    gain_settle,
    bias_settle,
    expert_ids,
    route_weight,
    expert_gate,
    expert_up,
    expert_down,
    gain_final,
    bias_final,
):
    rows = residual_in.shape[0]
    mine = lax.axis_index("sp")
    count = lax.axis_size("sp")
    heads_tp = lax.axis_size("tp")
    width_alpha = pairs_alpha.shape[2] // 2
    width_beta = pairs_beta.shape[2] // 2
    grouped_alpha = query_alpha.reshape(rows, pairs_alpha.shape[1], -1, width_alpha)
    grouped_beta = query_beta.reshape(rows, pairs_beta.shape[1], -1, width_beta)
    query_first = mine * rows
    initial = (
        jnp.zeros(grouped_alpha.shape, jnp.float32),
        jnp.zeros(grouped_beta.shape, jnp.float32),
        jnp.zeros((grouped_alpha.shape[1], grouped_alpha.shape[2], rows), jnp.float32),
        jnp.zeros((grouped_beta.shape[1], grouped_beta.shape[2], rows), jnp.float32),
    )

    def visit(state, pairs, offsets, key_first):
        acc_alpha, acc_beta, rest_alpha, rest_beta = state
        acc_alpha, rest_alpha = break_block(
            acc_alpha, rest_alpha, grouped_alpha, pairs[0], offsets[0], key_first, query_first
        )
        acc_beta, rest_beta = break_block(
            acc_beta, rest_beta, grouped_beta, pairs[1], offsets[1], key_first, query_first
        )
        return (acc_alpha, acc_beta, rest_alpha, rest_beta)

    def maybe_visit(state, turn, pairs, offsets):
        return lax.cond(
            turn <= mine,
            lambda kept: visit(kept, pairs, offsets, (mine - turn) * rows),
            lambda kept: kept,
            state,
        )

    pairs_all = (
        lax.all_gather(pairs_alpha, "sp", axis=0, tiled=True),
        lax.all_gather(pairs_beta, "sp", axis=0, tiled=True),
    )
    offsets_all = (
        lax.all_gather(offset_alpha, "sp", axis=0, tiled=True),
        lax.all_gather(offset_beta, "sp", axis=0, tiled=True),
    )

    def turn_all(turn, state):
        first_row = (mine - turn) * rows
        pairs = (
            lax.dynamic_slice_in_dim(pairs_all[0], first_row, rows, 0),
            lax.dynamic_slice_in_dim(pairs_all[1], first_row, rows, 0),
        )
        offsets = (
            lax.dynamic_slice_in_dim(offsets_all[0], first_row, rows, 0),
            lax.dynamic_slice_in_dim(offsets_all[1], first_row, rows, 0),
        )
        return maybe_visit(state, turn, pairs, offsets)

    state = lax.fori_loop(0, count, turn_all, initial)
    attend_alpha = state[0].reshape(rows, -1)
    attend_beta = state[1].reshape(rows, -1)
    squares = lax.psum(
        (jnp.sum(attend_alpha * attend_alpha, axis=1), jnp.sum(attend_beta * attend_beta, axis=1)),
        "tp",
    )
    scale_alpha = lax.rsqrt(squares[0] / (attend_alpha.shape[1] * heads_tp) + norm_eps)
    scale_beta = lax.rsqrt(squares[1] / (attend_beta.shape[1] * heads_tp) + norm_eps)
    normed_alpha = (attend_alpha * scale_alpha[:, None] * gain_alpha).astype(jnp.bfloat16)
    normed_beta = (attend_beta * scale_beta[:, None] * gain_beta).astype(jnp.bfloat16)
    term = jnp.dot(normed_alpha, project_alpha, preferred_element_type=jnp.float32) + jnp.dot(
        normed_beta, project_beta, preferred_element_type=jnp.float32
    )
    mixed = lax.psum_scatter(term.astype(jnp.bfloat16), "tp", scatter_dimension=1, tiled=True)
    columns = residual_in.shape[1] * heads_tp
    first = depth_scale * residual_in.astype(jnp.float32) + mixed.astype(jnp.float32)
    sums_one = lax.psum((jnp.sum(first, axis=1), jnp.sum(first * first, axis=1)), "tp")
    settled = finish_norm(first, sums_one, gain_settle, bias_settle, columns)
    cap = 3 * rows // count
    flat_ids = expert_ids.reshape(2 * rows)
    onehot = (flat_ids[:, None] == jnp.arange(count, dtype=jnp.int32)[None, :]).astype(jnp.int32)
    before = jnp.cumsum(onehot, axis=0, dtype=jnp.int32) - onehot
    slot = jnp.sum(before * onehot, axis=1, dtype=jnp.int32)
    place = flat_ids * cap + slot
    hit = place[None, :] == jnp.arange(count * cap, dtype=jnp.int32)[:, None]
    owner = jnp.arange(2 * rows, dtype=jnp.int32) // 2
    source = jnp.sum(jnp.where(hit, owner[None, :], 0), axis=1, dtype=jnp.int32)
    filled = jnp.any(hit, axis=1)
    gate_local = expert_gate[0]
    up_local = expert_up[0]
    send = jnp.where(filled[:, None], settled[source], jnp.zeros((), jnp.bfloat16)).reshape(
        count, cap, -1
    )
    arrived = lax.all_to_all(send, "sp", split_axis=0, concat_axis=0, tiled=True)
    piece = lax.all_gather(arrived, "tp", axis=2, tiled=True)
    flat = piece.reshape(-1, piece.shape[2])
    gate = jnp.dot(flat, gate_local, preferred_element_type=jnp.float32)
    up = jnp.dot(flat, up_local, preferred_element_type=jnp.float32)
    hidden = (jax.nn.silu(gate) * up).astype(jnp.bfloat16)
    partial_value = jnp.dot(hidden, expert_down[0], preferred_element_type=jnp.float32).reshape(
        count, cap, -1
    )
    summed = lax.psum_scatter(
        partial_value.astype(jnp.bfloat16), "tp", scatter_dimension=2, tiled=True
    )
    back = lax.all_to_all(summed, "sp", split_axis=0, concat_axis=0, tiled=True).reshape(
        count * cap, -1
    )
    picked = back[place].reshape(rows, 2, -1).astype(jnp.float32)
    routed = route_weight[:, 0:1] * picked[:, 0] + route_weight[:, 1:2] * picked[:, 1]
    second = depth_scale * settled.astype(jnp.float32) + routed
    sums_two = lax.psum((jnp.sum(second, axis=1), jnp.sum(second * second, axis=1)), "tp")
    return finish_norm(second, sums_two, gain_final, bias_final, columns)


GROUP_COUNT = 4
LANE = 128
BF = jnp.bfloat16
F32 = jnp.float32
LOG2E = 1.4426950408889634


def dot(a, b, dims=((1,), (0,))):
    return lax.dot_general(a, b, (dims, ((), ())), preferred_element_type=F32)


def thirds(v):
    hi = v.astype(BF).astype(F32)
    mid = (v - hi).astype(BF).astype(F32)
    return hi, mid, v - hi - mid


def iota(shape, dim):
    return lax.broadcasted_iota(jnp.int32, shape, dim)


def call(kernel, outs, args, vmem, scratch=(), hidden=0):
    local = pl.BlockSpec(memory_space=pltpu.VMEM)
    spare = pl.BlockSpec(memory_space=pl.ANY)
    return pl.pallas_call(
        kernel,
        out_shape=outs,
        in_specs=[local] * (len(args) - hidden) + [spare] * hidden,
        out_specs=[local] * len(outs),
        scratch_shapes=list(scratch),
        compiler_params=pltpu.CompilerParams(vmem_limit_bytes=vmem << 20),
    )(*args)


def spot():
    sp = lax.axis_index("sp")
    tp = lax.axis_index("tp")
    return sp // 2, sp % 2, tp


def in_hbm(*values):
    return tuple(pltpu.with_memory_space_constraint(v, pltpu.HBM) for v in values)


def shape_of(shape, dtype=BF):
    return jax.ShapeDtypeStruct(shape, dtype)


def route_kernel(cap, ids, weight, *refs):
    m_out, n_out, w_out = refs[-3:]
    z, _, t = spot()
    rows = ids.shape[1]
    first = iota((rows, rows), 0)
    second = iota((rows, rows), 1)

    def column(line):
        return jnp.sum(jnp.where(first == second, line, 0), axis=1, keepdims=True)

    grow = lax.shift_right_logical(ids[0:1, :], 1)
    gcol = column(grow)
    same = gcol == grow
    slot_col = jnp.sum(jnp.where(same & (second < first), 1, 0), axis=1, keepdims=True)
    slot_row = jnp.sum(jnp.where(same & (first < second), 1, 0), axis=0, keepdims=True)
    away = (grow ^ (2 * (z & 1))) ^ t
    block = 2 * (away & 1) + lax.shift_right_logical(away, 1)
    m = jnp.where(iota((4 * cap, rows), 0) == block * cap + slot_row, 1.0, 0.0).astype(BF)
    m_out[...] = m
    place = ((z + 4 - gcol) & 3) * cap + slot_col
    n_out[...] = jnp.where(iota((rows, 4 * cap), 1) == place, 1.0, 0.0).astype(BF)
    even = (ids[0:1, :] & 1) == 0
    w_even = column(jnp.where(even, weight[0:1, :], weight[1:2, :]))
    w_odd = column(jnp.where(even, weight[1:2, :], weight[0:1, :]))
    lane = iota((rows, LANE), 1)
    table = jnp.zeros((rows, LANE), F32)
    for k, part in enumerate(thirds(w_even) + thirds(w_odd)):
        table = jnp.where(lane == k, part, table)
    w_out[...] = dot(m[:cap], table.astype(BF)).astype(BF)


def pack_kernel(qa, ka, qb, kb, offs_a, offs_b, *outs):
    z, x, _ = spot()
    rows = qa.shape[0]
    planes = qa.shape[1] // LANE
    same, cross = outs[:planes], outs[planes:]

    def offset_rows(ref, values):
        parts = []
        for v in values:
            parts += list(thirds(v))
        parts += [jnp.zeros((1, LANE), F32)] * (8 - len(parts))
        block = jnp.concatenate(parts, axis=0).astype(BF)
        for k in range(ref.shape[1] // LANE):
            ref[pl.ds(rows, 8), k * LANE : (k + 1) * LANE] = block

    all_a = ka[...].astype(F32)
    all_b = kb[...].astype(F32)
    for u in range(planes):
        d = (u + planes - z) % planes
        cols = slice(u * LANE, (u + 1) * LANE)
        kv = all_a[:, u, :].astype(BF)
        kv_beta = all_b[:, u, :].astype(BF)
        for k in range(planes):

            @pl.when(d == k)
            def _():
                for flip in range(2):

                    @pl.when(x == flip)
                    def _():
                        alpha, beta = (cross[k], same[k]) if flip else (same[k], cross[k])
                        alpha[0:rows, 0:LANE] = qa[:, cols]
                        alpha[0:rows, LANE : 2 * LANE] = kv
                        offset_rows(alpha, [offs_a[2 * u : 2 * u + 1, :], offs_a[2 * u + 1 : 2 * u + 2, :]])
                        beta[0:rows, 0:LANE] = qb[:, cols]
                        beta[0:rows, LANE : 2 * LANE] = kv_beta[:, 0:LANE]
                        offset_rows(beta, [offs_b[u : u + 1, :]])
                        same[k][0:rows, 2 * LANE :] = kv_beta[:, LANE:]


def relay_kernel(*refs):
    out = refs[-1]
    rows = out.shape[0] // (len(refs) - 1)
    for d, ref in enumerate(refs[:-1]):
        out[d * rows : (d + 1) * rows, :] = ref[0:rows, 2 * LANE :]


def gather_kernel(planes, same, cross, relayed, q_s, k_s, v_s, off_s):
    z, x, _ = spot()
    rows = k_s.shape[0] // (2 * planes)
    half = LANE // 2
    low = iota((rows, LANE), 1) < half
    for d in range(planes):
        for ref, other in ((same[d], x), (cross[d], 1 - x)):
            p = (z + planes - d) % planes
            at = pl.ds(pl.multiple_of((2 * p + other) * rows, rows), rows)
            by_x = pl.ds(pl.multiple_of((planes * other + p) * rows, rows), rows)
            q = ref[0:rows, 0:LANE]
            zero = jnp.zeros_like(q)
            q_s[0, by_x, :] = jnp.where(low | (x != 0), q, zero)
            q_s[1, by_x, :] = jnp.where(low, zero, q)
            kv = ref[0:rows, LANE : 2 * LANE]
            turned = jnp.concatenate([kv[:, half:], kv[:, :half]], axis=1)
            values = relayed[d * rows : (d + 1) * rows, :] if ref is cross[d] else ref[0:rows, 2 * LANE :]
            k_s[at, :] = jnp.where(low | (x != 0), kv, turned)
            v_s[at, :] = jnp.where(x != 0, values, jnp.where(low, turned, kv))
            lines = ref[pl.ds(rows, 8), 0:LANE].astype(F32)
            for h in range(2):
                off_s[h : h + 1, at] = LOG2E * jnp.sum(lines[3 * h : 3 * h + 3], axis=0, keepdims=True)


def attend_half(planes, side, q_s, k_s, v_s, off_s, out, acc_s, rest_s, tri_s):
    z, x, _ = spot()
    rows = k_s.shape[0] // (2 * planes)
    tile = 2 * rows
    low = iota((rows, LANE), 1) < LANE // 2
    ti = iota((tile, tile), 0)
    tj = iota((tile, tile), 1)
    tri_s[...] = jnp.where(ti > tj, 1.0, 0.0).astype(BF)
    valid = (tj < ti + side * rows) | (ti >= rows)
    scale = jnp.where(x == 0, (LANE // 2) ** (-0.5) * LOG2E, LANE ** (-0.5) * LOG2E).astype(F32)
    base = side * (planes * rows)

    def one_head(h, carry):
        for j in range(planes - 1, -1, -1):
            cols = slice(j * tile, (j + 1) * tile)
            first = j * rows
            while first < planes * rows:
                count = min(tile, planes * rows - first)
                at = slice(first, first + count)
                diagonal = first == j * rows
                fresh = rows if diagonal else 0
                q = q_s[h, pl.ds(pl.multiple_of(base + first, rows), count), :]
                s = dot(q, k_s[cols, :], ((1,), (1,))) * scale + off_s[pl.ds(h, 1), cols]
                top = jnp.minimum(s, 64.0)
                take = top - jnp.log2(1.0 + jnp.exp2(top))
                soft = s - take
                if diagonal:
                    soft = jnp.where(valid[:count], soft, 0.0)
                soft = soft.astype(BF)
                after = dot(soft, tri_s[...])
                if fresh:
                    rest_s[first : first + rows, :] = jnp.zeros((rows, 1), F32)
                    acc_s[h, first : first + rows, :] = jnp.zeros((rows, LANE), F32)
                rest = rest_s[at, :]
                w = jnp.exp2(take - (after + rest))
                if diagonal:
                    w = jnp.where(valid[:count], w, 0.0)
                acc_s[h, at, :] = acc_s[h, at, :] + dot(w.astype(BF), v_s[cols, :])
                if j > 0:
                    rest_s[at, :] = rest + after[:, 0:1] + soft[:, 0:1].astype(F32)
                first += count
        return carry

    lax.fori_loop(0, jnp.where(x == 0, 2, 1), one_head, 0)
    for d in range(planes):
        at = pl.ds(pl.multiple_of(((z + d) % planes) * rows, rows), rows)
        value = jnp.where(low | (x != 0), acc_s[0, at, :], acc_s[1, at, :])
        out[d * rows : (d + 1) * rows, :] = value.astype(BF)


def attend_one_kernel(planes, spare, *refs):
    same, cross = refs[:planes], refs[planes : 2 * planes]
    refs = refs[2 * planes :]
    out, *held = refs[1 + spare : 6 + spare]
    gather_kernel(planes, same, cross, refs[0], *held)
    side = 1 - lax.axis_index("sp") % 2
    attend_half(planes, side, *held, out, *refs[6 + spare :])


def attend_two_kernel(planes, *refs):
    attend_half(planes, lax.axis_index("sp") % 2, *refs)


def merge_kernel(own, got, *outs):
    _, x, _ = spot()
    rows = own.shape[0] // len(outs)
    for d, ref in enumerate(outs):
        at = slice(d * rows, (d + 1) * rows)
        ref[:, pl.ds(pl.multiple_of(x * LANE, LANE), LANE)] = own[at]
        ref[:, pl.ds(pl.multiple_of((1 - x) * LANE, LANE), LANE)] = got[at]


def collect_kernel(planes, *refs):
    parts = refs[:planes]
    gains, out, sums = refs[planes:]
    z, _, _ = spot()
    width = planes * LANE
    lane = LANE
    for d in range(planes):
        u = (z + planes - d) % planes
        for k in range(2):
            at = pl.ds(pl.multiple_of(k * width + u * lane, lane), lane)
            out[:, at] = parts[d][:, k * lane : (k + 1) * lane]
    ones = jnp.ones((8, width), F32)
    whole = out[...].astype(F32)
    for k in range(2):
        part = whole[:, k * width : (k + 1) * width]
        line = lax.dot_general(
            ones,
            part * part,
            (((1,), (1,)), ((), ())),
            precision=lax.Precision.HIGHEST,
            preferred_element_type=F32,
        )
        sums[k : k + 1, :] = line[0:1]
    sums[2:8, :] = jnp.zeros((6, sums.shape[1]), F32)
    out[...] = (whole * gains[0:1, :]).astype(BF)


def project_kernel(columns, att, m, resid, s0, s1, s2, s3, pa, pb, keep, send, t_s):
    rows, width = resid.shape
    total = s0[0:2, :] + s1[0:2, :] + s2[0:2, :] + s3[0:2, :]
    factor = lax.rsqrt(total / columns + norm_eps)
    eye = iota((rows, rows), 0) == iota((rows, rows), 1)
    f_a = jnp.sum(jnp.where(eye, factor[0:1], 0.0), axis=1, keepdims=True)
    f_b = jnp.sum(jnp.where(eye, factor[1:2], 0.0), axis=1, keepdims=True)
    for k in range(columns // width):
        at = slice(k * width, (k + 1) * width)
        t_s[:, at] = dot(att[:, :width], pa[:, at]) * f_a + dot(att[:, width:], pb[:, at]) * f_b
    own = pl.ds(pl.multiple_of(lax.axis_index("tp") * width, LANE), width)
    t_s[:, own] = t_s[:, own] + depth_scale * resid[...].astype(F32)
    mid = keep.shape[0]
    for k in range(columns // width):
        at = slice(k * width, (k + 1) * width)
        moved = dot(m[...], t_s[:, at].astype(BF)).astype(BF)
        keep[:, at] = moved[:mid]
        send[:, at] = moved[mid:]


def pair_kernel(keep, got, own, send):
    n = own.shape[0]
    total = keep[...].astype(F32) + got[...].astype(F32)
    own[...] = total[:n]
    send[...] = total[n:].astype(BF)


def settle_kernel(own, got, w, l0, l1, l2, l3, out, lines):
    _, _, t = spot()
    width = l0.shape[1]
    for k, ref in enumerate((l0, l1, l2, l3)):
        lines[:, pl.ds(pl.multiple_of((t ^ k) * width, LANE), width)] = ref[...]
    columns = lines.shape[1]
    first = own[...] + got[...].astype(F32)
    out[:, 0:columns] = row_norm(first, lines[0:1, :], lines[1:2, :])
    out[:, columns : columns + LANE] = w[...]


def row_norm(total, gain, bias):
    columns = total.shape[1]
    mean = jnp.sum(total, axis=1, keepdims=True) / columns
    var = jnp.sum(total * total, axis=1, keepdims=True) / columns - mean * mean
    return ((total - mean) * lax.rsqrt(var + norm_eps) * gain + bias).astype(BF)


def expert_kernel(*refs):
    gate, up, down, near, far, x_s, acc_s, w_s = refs[-8:]
    count = x_s.shape[0] // refs[0].shape[0]
    pieces = refs[:count]
    step = pl.program_id(0)
    n = pieces[0].shape[0]
    columns = x_s.shape[1]

    @pl.when(step == 0)
    def _():
        odd = lax.axis_index("sp") % 2 != 0
        for k in range(count):
            at = slice(k * n, (k + 1) * n)
            x_s[at, :] = pieces[k][:, 0:columns]
            w = pieces[k][:, columns : columns + LANE].astype(F32)
            even_w = w[:, 0:1] + w[:, 1:2] + w[:, 2:3]
            odd_w = w[:, 3:4] + w[:, 4:5] + w[:, 5:6]
            w_s[at, :] = jnp.where(odd, odd_w, even_w)
        acc_s[...] = jnp.zeros_like(acc_s)

    x = x_s[...]
    g = dot(x, gate[0])
    u = dot(x, up[0])
    hidden = (g / (1.0 + jnp.exp(-g)) * u).astype(BF)
    acc_s[...] += dot(hidden, down[0])

    @pl.when(step == pl.num_programs(0) - 1)
    def _():
        mid = count // 2 * n
        width = near.shape[1] // 2
        _, _, t = spot()
        for k in range(2):
            cols = slice(k * width, (k + 1) * width)
            at = pl.ds(pl.multiple_of((t ^ (2 * k)) * width, LANE), width)
            near[:, cols] = (acc_s[:, at] * w_s[...]).astype(BF)
            at = pl.ds(pl.multiple_of((t ^ (2 * k + 1)) * width, LANE), width)
            far[0:mid, cols] = (acc_s[mid:, at] * w_s[mid:, :]).astype(BF)
            far[mid:, cols] = (acc_s[0:mid, at] * w_s[0:mid, :]).astype(BF)


def chip_kernel(spots, targets, near, got, *refs):
    width = near.shape[1] // 2
    count = len(spots)
    n = near.shape[0] // (2 * count)
    for dc in range(2):
        for k, (dx, dy) in enumerate(spots):
            rows = slice((count * dc + k) * n, (count * dc + k + 1) * n)
            for ry in range(2):
                ref = refs[targets.index((dx, ry))]
                cols = slice(ry * width, (ry + 1) * width)
                total = near[rows, cols].astype(F32) + got[rows, cols].astype(F32)
                q = 2 * dc + (dy ^ ry) if ref.shape[0] == 4 * n else dc
                ref[q * n : (q + 1) * n, :] = total.astype(ref.dtype)


def second_kernel(keep, gy, gx0, gx1, gxy0, gxy1, s0, s1, s2, s3, second, sums, routed_s):
    z, _, t = spot()
    n = s0.shape[0]
    width = keep.shape[1]
    at = pl.ds(pl.multiple_of(t * width, LANE), width)
    for q, ref in enumerate((s0, s1, s2, s3)):
        rows = slice(q * n, (q + 1) * n)
        side = slice((q >> 1) * n, ((q >> 1) + 1) * n)
        routed = keep[rows, :] + gy[rows, :].astype(F32)
        for part in (gx1, gxy1) if q & 1 else (gx0, gxy0):
            routed = routed + part[side, :].astype(F32)
        routed_s[rows, :] = routed + depth_scale * ref[:, at].astype(F32)
    for k in range(4):
        dc = (k >> 1) ^ (t & 1)
        dy = ((k & 1) ^ lax.shift_right_logical(z, 1)) ^ lax.shift_right_logical(t, 1)
        start = pl.multiple_of((2 * dc + dy) * n, 16)
        second[k * n : (k + 1) * n, :] = routed_s[pl.ds(start, n), :]
    value = second[...]
    ones = jnp.ones((8, width), F32)
    for k, part in enumerate((value, value * value)):
        line = lax.dot_general(
            ones,
            part,
            (((1,), (1,)), ((), ())),
            precision=lax.Precision.HIGHEST,
            preferred_element_type=F32,
        )
        sums[k : k + 1, 0 : 4 * n] = line[0:1]


def finish_kernel(columns, second, c0, c1, c2, c3, lines, f0, f1, f2, f3, all_s):
    z, _, _ = spot()
    n = f0.shape[0]
    total = c0[0:2, 0 : 4 * n] + c1[0:2, 0 : 4 * n] + c2[0:2, 0 : 4 * n] + c3[0:2, 0 : 4 * n]
    mean = total[0:1] / columns
    scale = lax.rsqrt(total[1:2] / columns - mean * mean + norm_eps)
    eye = iota((4 * n, 4 * n), 0) == iota((4 * n, 4 * n), 1)
    mean = jnp.sum(jnp.where(eye, mean, 0.0), axis=1, keepdims=True)
    scale = jnp.sum(jnp.where(eye, scale, 0.0), axis=1, keepdims=True)
    all_s[...] = ((second[...] - mean) * scale * lines[0:1, :] + lines[1:2, :]).astype(BF)
    for d, ref in enumerate((f0, f1, f2, f3)):
        start = pl.multiple_of(((z + d) & 3) * n, 16)
        ref[...] = all_s[pl.ds(start, n), :]


def load_kernel(*refs):
    count = (len(refs) - 1) // 2
    sems = refs[-1]
    copies = [
        pltpu.make_async_copy(refs[k], refs[count + k], sems.at[k]) for k in range(count)
    ]
    for copy in copies:
        copy.start()
    for copy in copies:
        copy.wait()


def place_kernel(n, f0, f1, f2, f3, out):
    total = dot(n[...], jnp.concatenate([f0[...], f1[...], f2[...], f3[...]], axis=0))
    out[...] = total.astype(BF)


def fast_body(
    chips,
    lanes,
    residual_in,
    query_alpha,
    pairs_alpha,
    offset_alpha,
    gain_alpha,
    query_beta,
    pairs_beta,
    offset_beta,
    gain_beta,
    project_alpha,
    project_beta,
    gain_settle,
    bias_settle,
    expert_ids,
    route_weight,
    expert_gate,
    expert_up,
    expert_down,
    gain_final,
    bias_final,
):
    rows, width = residual_in.shape
    planes = chips // 2
    columns = width * lanes
    cap = 3 * rows // chips

    def move(v, dest):
        perm = []
        for a in range(chips * lanes):
            s, t = divmod(a, lanes)
            to = dest(s // 2, s % 2, t)
            if to is not None:
                perm.append((a, (to[0] * 2 + to[1]) * lanes + to[2]))
        return lax.ppermute(v, ("sp", "tp"), perm)

    def shift(v, d, flip):
        return move(v, lambda z, x, t: ((z + d) % planes, x ^ flip, t))

    def swap_tp(v, k):
        return move(v, lambda z, x, t: (z, x, t ^ k))

    def across_tp(v):
        other_y = swap_tp(v, 2)
        return v, swap_tp(v, 1), other_y, swap_tp(other_y, 1)

    def swap_plane(v, dx, k):
        return move(v, lambda z, x, t: (z, x ^ dx, t ^ k))

    packed = call(
        pack_kernel,
        [shape_of((rows + 8, 3 * LANE))] * planes + [shape_of((rows + 8, 2 * LANE))] * planes,
        in_hbm(
            query_alpha,
            pairs_alpha,
            query_beta,
            pairs_beta,
            jnp.transpose(offset_alpha),
            jnp.transpose(offset_beta),
        ),
        12,
    )
    same, cross = packed[:planes], packed[planes:]
    got_same, got_cross = [same[0]] + [None] * (planes - 1), [None] * planes
    for d in (2, 1, 3):
        got_same[d] = shift(same[d], d, 0)
    for d in (2, 1, 3, 0):
        got_cross[d] = shift(cross[d], d, 1)
    (values,) = call(relay_kernel, [shape_of((planes * rows, LANE))], got_same, 4)
    relayed = swap_plane(values, 1, 0)

    m, n, w = call(
        lambda *refs: route_kernel(cap, *refs),
        [shape_of((4 * cap, rows)), shape_of((rows, 4 * cap)), shape_of((cap, LANE))],
        (*in_hbm(jnp.transpose(expert_ids), jnp.transpose(route_weight)), got_same[2]),
        8,
        hidden=1,
    )
    own_lines = jnp.stack([gain_settle, bias_settle])
    lines = [own_lines] + [swap_tp(own_lines, k) for k in range(1, 4)]

    def load(weights, after):
        count = len(weights)
        anywhere = pl.BlockSpec(memory_space=pl.ANY)
        return pl.pallas_call(
            lambda *refs: load_kernel(*refs[:count], *refs[count + 1 :]),
            out_shape=[shape_of(v.shape) for v in weights],
            in_specs=[anywhere] * (count + 1),
            out_specs=[pl.BlockSpec(memory_space=pltpu.VMEM)] * count,
            scratch_shapes=[pltpu.SemaphoreType.DMA((count,))],
            compiler_params=pltpu.CompilerParams(vmem_limit_bytes=16 << 20),
        )(*in_hbm(*weights), after)

    p_alpha, p_beta = load((project_alpha, project_beta), got_same[2])

    total = chips * rows
    spare = (m, n, w, *lines[1:], p_alpha)
    work = [
        pltpu.VMEM((2, planes * rows, LANE), F32),
        pltpu.VMEM((planes * rows, 1), F32),
        pltpu.VMEM((2 * rows, 2 * rows), BF),
    ]
    half = shape_of((planes * rows, LANE))
    other_x, *held = call(
        lambda *refs: attend_one_kernel(planes, len(spare), *refs),
        [half, shape_of((2, total, LANE)), shape_of((total, LANE)), shape_of((total, LANE)), shape_of((8, total), F32)],
        (*got_same, *got_cross, relayed, *spare),
        12,
        hidden=len(spare),
        scratch=work,
    )
    got_x = swap_plane(other_x, 1, 0)
    (own_x,) = call(
        lambda *refs: attend_two_kernel(planes, *refs), [half], tuple(held), 12, scratch=work
    )
    merged = call(merge_kernel, [shape_of((rows, 2 * LANE))] * planes, (own_x, got_x), 4)
    back = [merged[0]] + [shift(merged[d], d, 0) for d in range(1, planes)]
    gains = jnp.concatenate([gain_alpha, gain_beta])[None, :]
    att, sums = call(
        lambda *refs: collect_kernel(planes, *refs),
        [shape_of((rows, 2 * width)), shape_of((8, rows), F32)],
        (*back, gains),
        8,
    )
    all_sums = across_tp(sums)

    keep, send = call(
        lambda *refs: project_kernel(columns, *refs),
        [shape_of((2 * cap, columns))] * 2,
        (att, m, *in_hbm(residual_in), *all_sums, p_alpha, p_beta),
        12,
        scratch=[pltpu.VMEM((rows, columns), F32)],
    )
    own, send = call(
        pair_kernel,
        [shape_of((cap, columns), F32), shape_of((cap, columns))],
        (keep, swap_tp(send, 1)),
        8,
    )
    got = swap_tp(send, 2)
    e_gate, e_up, e_down = load((expert_gate, expert_up, expert_down), keep)
    settled, _ = call(
        settle_kernel,
        [shape_of((cap, columns + LANE)), shape_of((2, columns), F32)],
        (own, got, w, *lines),
        8,
    )

    def to_plane(z, x, t):
        g = t ^ (2 * (z & 1))
        return g, x, 2 * (t >> 1) + (z >> 1)

    mine = move(settled, to_plane)
    from_x, from_y, from_xy = (
        swap_plane(mine, 1, 0),
        swap_plane(mine, 0, 2),
        swap_plane(mine, 1, 2),
    )
    near = [mine, from_x, from_y]
    far = [swap_plane(mine, 0, 1)] + [swap_plane(v, 0, 1) for v in near[1:]]
    hidden = expert_gate.shape[2]
    chunk = hidden // 2

    def experts(pieces):
        n = len(pieces) * cap
        out = pl.BlockSpec((n, 2 * width), lambda j: (0, 0))
        return pl.pallas_call(
            expert_kernel,
            grid=(hidden // chunk,),
            out_shape=[shape_of((n, 2 * width))] * 2,
            in_specs=[pl.BlockSpec((cap, columns + LANE), lambda j: (0, 0))] * len(pieces)
            + [
                pl.BlockSpec((1, columns, chunk), lambda j: (0, 0, j)),
                pl.BlockSpec((1, columns, chunk), lambda j: (0, 0, j)),
                pl.BlockSpec((1, chunk, columns), lambda j: (0, j, 0)),
            ],
            out_specs=[out] * 2,
            scratch_shapes=[
                pltpu.VMEM((n, columns), BF),
                pltpu.VMEM((n, columns), F32),
                pltpu.VMEM((n, 1), F32),
            ],
            compiler_params=pltpu.CompilerParams(vmem_limit_bytes=24 << 20),
        )(*pieces, e_gate, e_up, e_down)

    def chip(spots, targets, outs, own, got):
        kernel = lambda *refs: chip_kernel(spots, targets, *refs)
        return call(kernel, outs, (own, got), 8)

    whole, side = shape_of((4 * cap, width)), shape_of((2 * cap, width))
    near_one, far_one = experts(near + far)
    keep, to_y, to_x0, to_xy0 = chip(
        ((0, 0), (1, 0), (0, 1)),
        ((0, 0), (0, 1), (1, 0), (1, 1)),
        [shape_of(whole.shape, F32), whole, side, side],
        near_one,
        swap_plane(far_one, 0, 1),
    )
    last, _ = lax.optimization_barrier((from_xy, far_one))
    near_two, far_two = experts([last, swap_plane(last, 0, 1)])
    to_x1, to_xy1 = chip(
        ((1, 1),), ((1, 0), (1, 1)), [side, side], near_two, swap_plane(far_two, 0, 1)
    )
    got_y = swap_plane(to_y, 0, 2)
    got_x0, got_x1 = swap_plane(to_x0, 1, 0), swap_plane(to_x1, 1, 0)
    got_xy1, got_xy0 = swap_plane(to_xy0, 1, 2), swap_plane(to_xy1, 1, 2)
    second, sums = call(
        second_kernel,
        [shape_of((4 * cap, width), F32), shape_of((8, 2 * LANE), F32)],
        (keep, got_y, got_x0, got_x1, got_xy0, got_xy1, near[0], near[2], far[0], far[2]),
        8,
        scratch=[pltpu.VMEM((4 * cap, width), F32)],
    )
    all_sums = across_tp(sums)
    ends = call(
        lambda *refs: finish_kernel(columns, *refs),
        [shape_of((cap, width))] * planes,
        (second, *all_sums, jnp.stack([gain_final, bias_final])),
        8,
        scratch=[pltpu.VMEM((4 * cap, width), BF)],
    )
    home = [ends[0]] + [shift(ends[d], d, 0) for d in range(1, planes)]
    (out,) = call(place_kernel, [shape_of((rows, width))], (n, *home), 4)
    return out


def solution(mesh):
    chips, lanes = mesh.shape["sp"], mesh.shape["tp"]

    def body(*args):
        residual_in, pairs_alpha, pairs_beta = args[0], args[2], args[6]
        planes = chips // 2
        fast = (
            chips // GROUP_COUNT == 2
            and lanes == planes
            and lanes == 4
            and pairs_alpha.shape[1] == planes
            and pairs_beta.shape[1] == planes
            and pairs_alpha.shape[2] == LANE
            and pairs_beta.shape[2] == 2 * LANE
            and residual_in.shape[0] == LANE
            and args[1].shape[1] == planes * LANE
            and args[5].shape[1] == planes * LANE
        )
        if not fast:
            return general_body(*args)
        return fast_body(chips, lanes, *args)

    in_specs = (
        P("sp", "tp"),
        P("sp", "tp"),
        P("sp", "tp", None),
        P("sp", "tp"),
        P("tp"),
        P("sp", "tp"),
        P("sp", "tp", None),
        P("sp", "tp"),
        P("tp"),
        P("tp", None),
        P("tp", None),
        P("tp"),
        P("tp"),
        P("sp", None),
        P("sp", None),
        P("sp", None, "tp"),
        P("sp", None, "tp"),
        P("sp", "tp", None),
        P("tp"),
        P("tp"),
    )
    out_specs = P("sp", "tp")
    return jax.shard_map(body, mesh=mesh, in_specs=in_specs, out_specs=out_specs, check_vma=False)
```

```python
import jax
import jax.numpy as jnp
from jax import lax
from jax.experimental import pallas as pl
from jax.experimental.pallas import tpu as pltpu
from jax.sharding import PartitionSpec as P


depth_scale = 2.0**0.5
norm_eps = 1e-05


def break_block(acc, remain, queries, pairs, offsets, key_first, query_first):
    width = queries.shape[3]
    keys = pairs[:, :, :width]
    values = pairs[:, :, width:]
    length = offsets.shape[0]
    kv_heads = queries.shape[1]
    share = queries.shape[2]
    scores = jnp.einsum(
        "qhrd,khd->hrqk", queries, keys, preferred_element_type=jnp.float32
    ) * width ** (-0.5)
    scores = (
        scores + jnp.transpose(offsets.reshape(length, kv_heads, share), (1, 2, 0))[:, :, None, :]
    )
    query_pos = query_first + jnp.arange(queries.shape[0], dtype=jnp.int32)
    key_pos = key_first + jnp.arange(length, dtype=jnp.int32)
    valid = key_pos[None, :] < query_pos[:, None]
    soft = jnp.where(valid, jax.nn.softplus(scores), 0.0)
    later = lax.cumsum(soft, axis=3, reverse=True) - soft
    weights = jnp.where(
        valid, jnp.exp(jax.nn.log_sigmoid(scores) - later + remain[..., None]), 0.0
    ).astype(jnp.bfloat16)
    acc = acc + jnp.einsum("hrqk,khd->qhrd", weights, values, preferred_element_type=jnp.float32)
    return (acc, remain - jnp.sum(soft, axis=3))


def finish_norm(total, sums, gain, bias, columns):
    mean = sums[0] / columns
    var = sums[1] / columns - mean * mean
    return ((total - mean[:, None]) * lax.rsqrt(var + norm_eps)[:, None] * gain + bias).astype(
        jnp.bfloat16
    )


def general_body(
    residual_in,
    query_alpha,
    pairs_alpha,
    offset_alpha,
    gain_alpha,
    query_beta,
    pairs_beta,
    offset_beta,
    gain_beta,
    project_alpha,
    project_beta,
    gain_settle,
    bias_settle,
    expert_ids,
    route_weight,
    expert_gate,
    expert_up,
    expert_down,
    gain_final,
    bias_final,
):
    rows = residual_in.shape[0]
    mine = lax.axis_index("sp")
    count = lax.axis_size("sp")
    heads_tp = lax.axis_size("tp")
    width_alpha = pairs_alpha.shape[2] // 2
    width_beta = pairs_beta.shape[2] // 2
    grouped_alpha = query_alpha.reshape(rows, pairs_alpha.shape[1], -1, width_alpha)
    grouped_beta = query_beta.reshape(rows, pairs_beta.shape[1], -1, width_beta)
    query_first = mine * rows
    initial = (
        jnp.zeros(grouped_alpha.shape, jnp.float32),
        jnp.zeros(grouped_beta.shape, jnp.float32),
        jnp.zeros((grouped_alpha.shape[1], grouped_alpha.shape[2], rows), jnp.float32),
        jnp.zeros((grouped_beta.shape[1], grouped_beta.shape[2], rows), jnp.float32),
    )

    def visit(state, pairs, offsets, key_first):
        acc_alpha, acc_beta, rest_alpha, rest_beta = state
        acc_alpha, rest_alpha = break_block(
            acc_alpha, rest_alpha, grouped_alpha, pairs[0], offsets[0], key_first, query_first
        )
        acc_beta, rest_beta = break_block(
            acc_beta, rest_beta, grouped_beta, pairs[1], offsets[1], key_first, query_first
        )
        return (acc_alpha, acc_beta, rest_alpha, rest_beta)

    def maybe_visit(state, turn, pairs, offsets):
        return lax.cond(
            turn <= mine,
            lambda kept: visit(kept, pairs, offsets, (mine - turn) * rows),
            lambda kept: kept,
            state,
        )

    pairs_all = (
        lax.all_gather(pairs_alpha, "sp", axis=0, tiled=True),
        lax.all_gather(pairs_beta, "sp", axis=0, tiled=True),
    )
    offsets_all = (
        lax.all_gather(offset_alpha, "sp", axis=0, tiled=True),
        lax.all_gather(offset_beta, "sp", axis=0, tiled=True),
    )

    def turn_all(turn, state):
        first_row = (mine - turn) * rows
        pairs = (
            lax.dynamic_slice_in_dim(pairs_all[0], first_row, rows, 0),
            lax.dynamic_slice_in_dim(pairs_all[1], first_row, rows, 0),
        )
        offsets = (
            lax.dynamic_slice_in_dim(offsets_all[0], first_row, rows, 0),
            lax.dynamic_slice_in_dim(offsets_all[1], first_row, rows, 0),
        )
        return maybe_visit(state, turn, pairs, offsets)

    state = lax.fori_loop(0, count, turn_all, initial)
    attend_alpha = state[0].reshape(rows, -1)
    attend_beta = state[1].reshape(rows, -1)
    squares = lax.psum(
        (jnp.sum(attend_alpha * attend_alpha, axis=1), jnp.sum(attend_beta * attend_beta, axis=1)),
        "tp",
    )
    scale_alpha = lax.rsqrt(squares[0] / (attend_alpha.shape[1] * heads_tp) + norm_eps)
    scale_beta = lax.rsqrt(squares[1] / (attend_beta.shape[1] * heads_tp) + norm_eps)
    normed_alpha = (attend_alpha * scale_alpha[:, None] * gain_alpha).astype(jnp.bfloat16)
    normed_beta = (attend_beta * scale_beta[:, None] * gain_beta).astype(jnp.bfloat16)
    term = jnp.dot(normed_alpha, project_alpha, preferred_element_type=jnp.float32) + jnp.dot(
        normed_beta, project_beta, preferred_element_type=jnp.float32
    )
    mixed = lax.psum_scatter(term.astype(jnp.bfloat16), "tp", scatter_dimension=1, tiled=True)
    columns = residual_in.shape[1] * heads_tp
    first = depth_scale * residual_in.astype(jnp.float32) + mixed.astype(jnp.float32)
    sums_one = lax.psum((jnp.sum(first, axis=1), jnp.sum(first * first, axis=1)), "tp")
    settled = finish_norm(first, sums_one, gain_settle, bias_settle, columns)
    cap = 3 * rows // count
    flat_ids = expert_ids.reshape(2 * rows)
    onehot = (flat_ids[:, None] == jnp.arange(count, dtype=jnp.int32)[None, :]).astype(jnp.int32)
    before = jnp.cumsum(onehot, axis=0, dtype=jnp.int32) - onehot
    slot = jnp.sum(before * onehot, axis=1, dtype=jnp.int32)
    place = flat_ids * cap + slot
    hit = place[None, :] == jnp.arange(count * cap, dtype=jnp.int32)[:, None]
    owner = jnp.arange(2 * rows, dtype=jnp.int32) // 2
    source = jnp.sum(jnp.where(hit, owner[None, :], 0), axis=1, dtype=jnp.int32)
    filled = jnp.any(hit, axis=1)
    gate_local = expert_gate[0]
    up_local = expert_up[0]
    send = jnp.where(filled[:, None], settled[source], jnp.zeros((), jnp.bfloat16)).reshape(
        count, cap, -1
    )
    arrived = lax.all_to_all(send, "sp", split_axis=0, concat_axis=0, tiled=True)
    piece = lax.all_gather(arrived, "tp", axis=2, tiled=True)
    flat = piece.reshape(-1, piece.shape[2])
    gate = jnp.dot(flat, gate_local, preferred_element_type=jnp.float32)
    up = jnp.dot(flat, up_local, preferred_element_type=jnp.float32)
    hidden = (jax.nn.silu(gate) * up).astype(jnp.bfloat16)
    partial_value = jnp.dot(hidden, expert_down[0], preferred_element_type=jnp.float32).reshape(
        count, cap, -1
    )
    summed = lax.psum_scatter(
        partial_value.astype(jnp.bfloat16), "tp", scatter_dimension=2, tiled=True
    )
    back = lax.all_to_all(summed, "sp", split_axis=0, concat_axis=0, tiled=True).reshape(
        count * cap, -1
    )
    picked = back[place].reshape(rows, 2, -1).astype(jnp.float32)
    routed = route_weight[:, 0:1] * picked[:, 0] + route_weight[:, 1:2] * picked[:, 1]
    second = depth_scale * settled.astype(jnp.float32) + routed
    sums_two = lax.psum((jnp.sum(second, axis=1), jnp.sum(second * second, axis=1)), "tp")
    return finish_norm(second, sums_two, gain_final, bias_final, columns)


GROUP_COUNT = 4
LANE = 128
BF = jnp.bfloat16
F32 = jnp.float32
LOG2E = 1.4426950408889634


def dot(a, b, dims=((1,), (0,))):
    return lax.dot_general(a, b, (dims, ((), ())), preferred_element_type=F32)


def thirds(v):
    hi = v.astype(BF).astype(F32)
    mid = (v - hi).astype(BF).astype(F32)
    return hi, mid, v - hi - mid


def iota(shape, dim):
    return lax.broadcasted_iota(jnp.int32, shape, dim)


def call(kernel, outs, args, vmem, scratch=(), hidden=0):
    local = pl.BlockSpec(memory_space=pltpu.VMEM)
    spare = pl.BlockSpec(memory_space=pl.ANY)
    return pl.pallas_call(
        kernel,
        out_shape=outs,
        in_specs=[local] * (len(args) - hidden) + [spare] * hidden,
        out_specs=[local] * len(outs),
        scratch_shapes=list(scratch),
        compiler_params=pltpu.CompilerParams(vmem_limit_bytes=vmem << 20),
    )(*args)


def spot():
    sp = lax.axis_index("sp")
    tp = lax.axis_index("tp")
    return sp // 2, sp % 2, tp


def in_hbm(*values):
    return tuple(pltpu.with_memory_space_constraint(v, pltpu.HBM) for v in values)


def shape_of(shape, dtype=BF):
    return jax.ShapeDtypeStruct(shape, dtype)


def route_kernel(cap, ids, weight, *refs):
    m_out, n_out, w_out = refs[-3:]
    z, _, t = spot()
    rows = ids.shape[1]
    first = iota((rows, rows), 0)
    second = iota((rows, rows), 1)

    def column(line):
        return jnp.sum(jnp.where(first == second, line, 0), axis=1, keepdims=True)

    grow = lax.shift_right_logical(ids[0:1, :], 1)
    gcol = column(grow)
    same = gcol == grow
    slot_col = jnp.sum(jnp.where(same & (second < first), 1, 0), axis=1, keepdims=True)
    slot_row = jnp.sum(jnp.where(same & (first < second), 1, 0), axis=0, keepdims=True)
    away = (grow ^ (2 * (z & 1))) ^ t
    block = 2 * (away & 1) + lax.shift_right_logical(away, 1)
    m = jnp.where(iota((4 * cap, rows), 0) == block * cap + slot_row, 1.0, 0.0).astype(BF)
    m_out[...] = m
    place = ((z + 4 - gcol) & 3) * cap + slot_col
    n_out[...] = jnp.where(iota((rows, 4 * cap), 1) == place, 1.0, 0.0).astype(BF)
    even = (ids[0:1, :] & 1) == 0
    w_even = column(jnp.where(even, weight[0:1, :], weight[1:2, :]))
    w_odd = column(jnp.where(even, weight[1:2, :], weight[0:1, :]))
    lane = iota((rows, LANE), 1)
    table = jnp.zeros((rows, LANE), F32)
    for k, part in enumerate(thirds(w_even) + thirds(w_odd)):
        table = jnp.where(lane == k, part, table)
    w_out[...] = dot(m[:cap], table.astype(BF)).astype(BF)


def pack_kernel(side, qa, ka, qb, kb, offs_a, offs_b, *outs):
    z, x, _ = spot()
    rows = qa.shape[0]
    planes = qa.shape[1] // LANE

    def offset_rows(ref, values):
        parts = []
        for v in values:
            parts += list(thirds(v))
        parts += [jnp.zeros((1, LANE), F32)] * (8 - len(parts))
        block = jnp.concatenate(parts, axis=0).astype(BF)
        for k in range(ref.shape[1] // LANE):
            ref[pl.ds(rows, 8), k * LANE : (k + 1) * LANE] = block

    all_a = ka[...].astype(F32)
    all_b = kb[...].astype(F32)
    for u in range(planes):
        d = (u + planes - z) % planes
        cols = slice(u * LANE, (u + 1) * LANE)
        kv = all_a[:, u, :].astype(BF)
        kv_beta = all_b[:, u, :].astype(BF)
        for k, ref in enumerate(outs):

            @pl.when((d == k) & (x == side))
            def _():
                ref[0:rows, 0:LANE] = qa[:, cols]
                ref[0:rows, LANE : 2 * LANE] = kv
                offset_rows(ref, [offs_a[2 * u : 2 * u + 1, :], offs_a[2 * u + 1 : 2 * u + 2, :]])

            @pl.when((d == k) & (x != side))
            def _():
                ref[0:rows, 0:LANE] = qb[:, cols]
                ref[0:rows, LANE : 2 * LANE] = kv_beta[:, 0:LANE]
                offset_rows(ref, [offs_b[u : u + 1, :]])

            if side == 0:

                @pl.when(d == k)
                def _():
                    ref[0:rows, 2 * LANE :] = kv_beta[:, LANE:]


def relay_kernel(*refs):
    out = refs[-1]
    rows = out.shape[0] // (len(refs) - 1)
    for d, ref in enumerate(refs[:-1]):
        out[d * rows : (d + 1) * rows, :] = ref[0:rows, 2 * LANE :]


def gather_kernel(planes, same, cross, relayed, q_s, k_s, v_s, off_s):
    z, x, _ = spot()
    rows = k_s.shape[0] // (2 * planes)
    half = LANE // 2
    low = iota((rows, LANE), 1) < half
    for d in range(planes):
        for ref, other in ((same[d], x), (cross[d], 1 - x)):
            p = (z + planes - d) % planes
            at = pl.ds(pl.multiple_of((2 * p + other) * rows, rows), rows)
            by_x = pl.ds(pl.multiple_of((planes * other + p) * rows, rows), rows)
            q = ref[0:rows, 0:LANE]
            zero = jnp.zeros_like(q)
            q_s[0, by_x, :] = jnp.where(low | (x != 0), q, zero)
            q_s[1, by_x, :] = jnp.where(low, zero, q)
            kv = ref[0:rows, LANE : 2 * LANE]
            turned = jnp.concatenate([kv[:, half:], kv[:, :half]], axis=1)
            values = relayed[d * rows : (d + 1) * rows, :] if ref is cross[d] else ref[0:rows, 2 * LANE :]
            k_s[at, :] = jnp.where(low | (x != 0), kv, turned)
            v_s[at, :] = jnp.where(x != 0, values, jnp.where(low, turned, kv))
            lines = ref[pl.ds(rows, 8), 0:LANE].astype(F32)
            for h in range(2):
                off_s[h : h + 1, at] = LOG2E * jnp.sum(lines[3 * h : 3 * h + 3], axis=0, keepdims=True)


def attend_half(planes, side, q_s, k_s, v_s, off_s, out, acc_s, tri_s):
    z, x, _ = spot()
    rows = k_s.shape[0] // (2 * planes)
    tile = 2 * rows
    low = iota((rows, LANE), 1) < LANE // 2
    ti = iota((tile, tile), 0)
    tj = iota((tile, tile), 1)
    tri_s[...] = jnp.where(ti > tj, 1.0, 0.0).astype(BF)
    valid = (tj < ti + side * rows) | (ti >= rows)
    scale = jnp.where(x == 0, (LANE // 2) ** (-0.5) * LOG2E, LANE ** (-0.5) * LOG2E).astype(F32)
    base = side * (planes * rows)

    def run(heads):
        tasks = []
        for j in range(planes - 1, -1, -1):
            for first in range(j, planes, 2):
                tasks += [(h, j, first, min(2, planes - first)) for h in range(heads)]
        rest = {}

        def product(task):
            h, j, first, count = task
            cols = slice(j * tile, (j + 1) * tile)
            at = pl.ds(pl.multiple_of(base + first * rows, rows), count * rows)
            return dot(q_s[h, at, :], k_s[cols, :], ((1,), (1,)))

        def suffix(task, s):
            h, j, first, count = task
            s = s * scale + off_s[h : h + 1, j * tile : (j + 1) * tile]
            top = jnp.minimum(s, 64.0)
            take = top - jnp.log2(1.0 + jnp.exp2(top))
            soft = s - take
            if first == j:
                soft = jnp.where(valid[: count * rows], soft, 0.0)
            soft = soft.astype(BF)
            after = dot(soft, tri_s[...])
            return take, after, soft[:, 0:1].astype(F32)

        def gather(task, take, after, own):
            h, j, first, count = task
            fresh = first == j
            blocks = range(first, first + count)
            zero = jnp.zeros((rows, 1), F32)
            before = [rest.get((h, i), zero) for i in blocks]
            before = before[0] if count == 1 else jnp.concatenate(before, axis=0)
            w = jnp.exp2(take - (after + before))
            if fresh:
                w = jnp.where(valid[: count * rows], w, 0.0)
            part = dot(w.astype(BF), v_s[j * tile : (j + 1) * tile, :])
            total = before + after[:, 0:1] + own
            for k, i in enumerate(blocks):
                at = slice(i * rows, (i + 1) * rows)
                piece = part[k * rows : (k + 1) * rows]
                acc_s[h, at, :] = piece if i == j else acc_s[h, at, :] + piece
                rest[(h, i)] = total[k * rows : (k + 1) * rows]

        count = len(tasks)
        ahead, middle = {}, {}
        for n in range(count + 2):
            if n < count:
                ahead[n] = product(tasks[n])
            if 0 <= n - 1 < count:
                middle[n - 1] = suffix(tasks[n - 1], ahead.pop(n - 1))
            if 0 <= n - 2:
                gather(tasks[n - 2], *middle.pop(n - 2))

    @pl.when(x == 0)
    def _():
        run(2)

    @pl.when(x != 0)
    def _():
        run(1)

    for d in range(planes):
        at = pl.ds(pl.multiple_of(((z + d) % planes) * rows, rows), rows)
        value = jnp.where(low | (x != 0), acc_s[0, at, :], acc_s[1, at, :])
        out[d * rows : (d + 1) * rows, :] = value.astype(BF)


def attend_one_kernel(planes, spare, *refs):
    same, cross = refs[:planes], refs[planes : 2 * planes]
    refs = refs[2 * planes :]
    out, *held = refs[1 + spare : 6 + spare]
    gather_kernel(planes, same, cross, refs[0], *held)
    side = 1 - lax.axis_index("sp") % 2
    attend_half(planes, side, *held, out, *refs[6 + spare :])


def attend_two_kernel(planes, *refs):
    attend_half(planes, lax.axis_index("sp") % 2, *refs)


def merge_kernel(own, got, *outs):
    _, x, _ = spot()
    rows = own.shape[0] // len(outs)
    for d, ref in enumerate(outs):
        at = slice(d * rows, (d + 1) * rows)
        ref[:, pl.ds(pl.multiple_of(x * LANE, LANE), LANE)] = own[at]
        ref[:, pl.ds(pl.multiple_of((1 - x) * LANE, LANE), LANE)] = got[at]


def collect_kernel(planes, *refs):
    parts = refs[:planes]
    gains, out, sums = refs[planes:]
    z, _, _ = spot()
    width = planes * LANE
    lane = LANE
    for d in range(planes):
        u = (z + planes - d) % planes
        for k in range(2):
            at = pl.ds(pl.multiple_of(k * width + u * lane, lane), lane)
            out[:, at] = parts[d][:, k * lane : (k + 1) * lane]
    ones = jnp.ones((8, width), F32)
    whole = out[...].astype(F32)
    for k in range(2):
        part = whole[:, k * width : (k + 1) * width]
        line = lax.dot_general(
            ones,
            part * part,
            (((1,), (1,)), ((), ())),
            precision=lax.Precision.HIGHEST,
            preferred_element_type=F32,
        )
        sums[k : k + 1, :] = line[0:1]
    sums[2:8, :] = jnp.zeros((6, sums.shape[1]), F32)
    out[...] = (whole * gains[0:1, :]).astype(BF)


def project_kernel(columns, att, m, resid, s0, s1, s2, s3, pa, pb, keep, send, t_s):
    rows, width = resid.shape
    total = s0[0:2, :] + s1[0:2, :] + s2[0:2, :] + s3[0:2, :]
    factor = lax.rsqrt(total / columns + norm_eps)
    eye = iota((rows, rows), 0) == iota((rows, rows), 1)
    f_a = jnp.sum(jnp.where(eye, factor[0:1], 0.0), axis=1, keepdims=True)
    f_b = jnp.sum(jnp.where(eye, factor[1:2], 0.0), axis=1, keepdims=True)
    for k in range(columns // width):
        at = slice(k * width, (k + 1) * width)
        t_s[:, at] = dot(att[:, :width], pa[:, at]) * f_a + dot(att[:, width:], pb[:, at]) * f_b
    own = pl.ds(pl.multiple_of(lax.axis_index("tp") * width, LANE), width)
    t_s[:, own] = t_s[:, own] + depth_scale * resid[...].astype(F32)
    mid = keep.shape[0]
    for k in range(columns // width):
        at = slice(k * width, (k + 1) * width)
        moved = dot(m[...], t_s[:, at].astype(BF)).astype(BF)
        keep[:, at] = moved[:mid]
        send[:, at] = moved[mid:]


def pair_kernel(keep, got, own, send):
    n = own.shape[0]
    total = keep[...].astype(F32) + got[...].astype(F32)
    own[...] = total[:n]
    send[...] = total[n:].astype(BF)


def settle_kernel(own, got, w, l0, l1, l2, l3, out, lines):
    _, _, t = spot()
    width = l0.shape[1]
    for k, ref in enumerate((l0, l1, l2, l3)):
        lines[:, pl.ds(pl.multiple_of((t ^ k) * width, LANE), width)] = ref[...]
    columns = lines.shape[1]
    first = own[...] + got[...].astype(F32)
    out[:, 0:columns] = row_norm(first, lines[0:1, :], lines[1:2, :])
    out[:, columns : columns + LANE] = w[...]


def row_norm(total, gain, bias):
    columns = total.shape[1]
    mean = jnp.sum(total, axis=1, keepdims=True) / columns
    var = jnp.sum(total * total, axis=1, keepdims=True) / columns - mean * mean
    return ((total - mean) * lax.rsqrt(var + norm_eps) * gain + bias).astype(BF)


def expert_kernel(*refs):
    gate, up, down, near, far, x_s, h_s, w_s = refs[-8:]
    n = refs[0].shape[0]
    count = x_s.shape[0] // n
    columns = x_s.shape[1]
    odd = lax.axis_index("sp") % 2 != 0
    _, _, t = spot()
    for k, piece in enumerate(refs[:count]):
        at = slice(k * n, (k + 1) * n)
        x_s[at, :] = piece[:, 0:columns]
        w = piece[:, columns : columns + LANE].astype(F32)
        even_w = w[:, 0:1] + w[:, 1:2] + w[:, 2:3]
        odd_w = w[:, 3:4] + w[:, 4:5] + w[:, 5:6]
        w_s[at, :] = jnp.where(odd, odd_w, even_w)

    x = x_s[...]
    chunk = 2 * LANE
    chunks = h_s.shape[1] // chunk
    ahead = None
    for k in range(chunks + 1):
        this = None
        if k < chunks:
            at = slice(k * chunk, (k + 1) * chunk)
            this = dot(x, gate[0, :, at]), dot(x, up[0, :, at])
        if ahead is not None:
            g, u = ahead
            h_s[:, (k - 1) * chunk : k * chunk] = (g / (1.0 + jnp.exp(-g)) * u).astype(BF)
        ahead = this

    mid = count // 2 * n
    width = near.shape[1] // 2
    for k in range(2):
        cols = slice(k * width, (k + 1) * width)
        at = pl.ds(pl.multiple_of((t ^ (2 * k + 1)) * width, LANE), width)
        value = (dot(h_s[...], down[0, :, at]) * w_s[...]).astype(BF)
        far[0:mid, cols] = value[mid:]
        far[mid:, cols] = value[:mid]
        at = pl.ds(pl.multiple_of((t ^ (2 * k)) * width, LANE), width)
        near[:, cols] = (dot(h_s[...], down[0, :, at]) * w_s[...]).astype(BF)


def chip_kernel(spots, targets, near, got, *refs):
    width = near.shape[1] // 2
    count = len(spots)
    n = near.shape[0] // (2 * count)
    for dc in range(2):
        for k, (dx, dy) in enumerate(spots):
            rows = slice((count * dc + k) * n, (count * dc + k + 1) * n)
            for ry in range(2):
                ref = refs[targets.index((dx, ry))]
                cols = slice(ry * width, (ry + 1) * width)
                total = near[rows, cols].astype(F32) + got[rows, cols].astype(F32)
                q = 2 * dc + (dy ^ ry) if ref.shape[0] == 4 * n else dc
                ref[q * n : (q + 1) * n, :] = total.astype(ref.dtype)


def second_kernel(keep, gy, gx0, gx1, gxy0, gxy1, s0, s1, s2, s3, second, sums, routed_s):
    z, _, t = spot()
    n = s0.shape[0]
    width = keep.shape[1]
    at = pl.ds(pl.multiple_of(t * width, LANE), width)
    for q, ref in enumerate((s0, s1, s2, s3)):
        rows = slice(q * n, (q + 1) * n)
        side = slice((q >> 1) * n, ((q >> 1) + 1) * n)
        routed = keep[rows, :] + gy[rows, :].astype(F32)
        for part in (gx1, gxy1) if q & 1 else (gx0, gxy0):
            routed = routed + part[side, :].astype(F32)
        routed_s[rows, :] = routed + depth_scale * ref[:, at].astype(F32)
    for k in range(4):
        dc = (k >> 1) ^ (t & 1)
        dy = ((k & 1) ^ lax.shift_right_logical(z, 1)) ^ lax.shift_right_logical(t, 1)
        start = pl.multiple_of((2 * dc + dy) * n, 16)
        second[k * n : (k + 1) * n, :] = routed_s[pl.ds(start, n), :]
    value = second[...]
    ones = jnp.ones((8, width), F32)
    for k, part in enumerate((value, value * value)):
        line = lax.dot_general(
            ones,
            part,
            (((1,), (1,)), ((), ())),
            precision=lax.Precision.HIGHEST,
            preferred_element_type=F32,
        )
        sums[k : k + 1, 0 : 4 * n] = line[0:1]


def finish_kernel(columns, second, c0, c1, c2, c3, lines, f0, f1, f2, f3, all_s):
    z, _, _ = spot()
    n = f0.shape[0]
    total = c0[0:2, 0 : 4 * n] + c1[0:2, 0 : 4 * n] + c2[0:2, 0 : 4 * n] + c3[0:2, 0 : 4 * n]
    mean = total[0:1] / columns
    scale = lax.rsqrt(total[1:2] / columns - mean * mean + norm_eps)
    eye = iota((4 * n, 4 * n), 0) == iota((4 * n, 4 * n), 1)
    mean = jnp.sum(jnp.where(eye, mean, 0.0), axis=1, keepdims=True)
    scale = jnp.sum(jnp.where(eye, scale, 0.0), axis=1, keepdims=True)
    all_s[...] = ((second[...] - mean) * scale * lines[0:1, :] + lines[1:2, :]).astype(BF)
    for d, ref in enumerate((f0, f1, f2, f3)):
        start = pl.multiple_of(((z + d) & 3) * n, 16)
        ref[...] = all_s[pl.ds(start, n), :]


def load_kernel(*refs):
    count = (len(refs) - 1) // 2
    sems = refs[-1]
    copies = [
        pltpu.make_async_copy(refs[k], refs[count + k], sems.at[k]) for k in range(count)
    ]
    for copy in copies:
        copy.start()
    for copy in copies:
        copy.wait()


def place_kernel(n, f0, f1, f2, f3, out):
    total = dot(n[...], jnp.concatenate([f0[...], f1[...], f2[...], f3[...]], axis=0))
    out[...] = total.astype(BF)


def fast_body(
    chips,
    lanes,
    residual_in,
    query_alpha,
    pairs_alpha,
    offset_alpha,
    gain_alpha,
    query_beta,
    pairs_beta,
    offset_beta,
    gain_beta,
    project_alpha,
    project_beta,
    gain_settle,
    bias_settle,
    expert_ids,
    route_weight,
    expert_gate,
    expert_up,
    expert_down,
    gain_final,
    bias_final,
):
    rows, width = residual_in.shape
    planes = chips // 2
    columns = width * lanes
    cap = 3 * rows // chips

    def move(v, dest):
        perm = []
        for a in range(chips * lanes):
            s, t = divmod(a, lanes)
            to = dest(s // 2, s % 2, t)
            if to is not None:
                perm.append((a, (to[0] * 2 + to[1]) * lanes + to[2]))
        return lax.ppermute(v, ("sp", "tp"), perm)

    def shift(v, d, flip):
        return move(v, lambda z, x, t: ((z + d) % planes, x ^ flip, t))

    def swap_tp(v, k):
        return move(v, lambda z, x, t: (z, x, t ^ k))

    def across_tp(v):
        return v, swap_tp(v, 1), swap_tp(v, 2), swap_tp(v, 3)

    def swap_plane(v, dx, k):
        return move(v, lambda z, x, t: (z, x ^ dx, t ^ k))

    inputs = in_hbm(
        query_alpha,
        pairs_alpha,
        query_beta,
        pairs_beta,
        jnp.transpose(offset_alpha),
        jnp.transpose(offset_beta),
    )
    same, cross = (
        call(
            lambda *refs: pack_kernel(flip, *refs),
            [shape_of((rows + 8, (3 - flip) * LANE))] * planes,
            inputs,
            12,
        )
        for flip in range(2)
    )
    got_same, got_cross = [same[0]] + [None] * (planes - 1), [None] * planes
    for d in (2, 1, 3):
        got_same[d] = shift(same[d], d, 0)
    for d in (2, 1, 3, 0):
        got_cross[d] = shift(cross[d], d, 1)
    (values,) = call(relay_kernel, [shape_of((planes * rows, LANE))], got_same, 4)
    relayed = swap_plane(values, 1, 0)

    m, n, w = call(
        lambda *refs: route_kernel(cap, *refs),
        [shape_of((4 * cap, rows)), shape_of((rows, 4 * cap)), shape_of((cap, LANE))],
        (*in_hbm(jnp.transpose(expert_ids), jnp.transpose(route_weight)), got_same[2]),
        8,
        hidden=1,
    )
    own_lines = jnp.stack([gain_settle, bias_settle])
    lines = [own_lines] + [swap_tp(own_lines, k) for k in range(1, 4)]

    def load(weights, after):
        count = len(weights)
        anywhere = pl.BlockSpec(memory_space=pl.ANY)
        return pl.pallas_call(
            lambda *refs: load_kernel(*refs[:count], *refs[count + 1 :]),
            out_shape=[shape_of(v.shape) for v in weights],
            in_specs=[anywhere] * (count + 1),
            out_specs=[pl.BlockSpec(memory_space=pltpu.VMEM)] * count,
            scratch_shapes=[pltpu.SemaphoreType.DMA((count,))],
            compiler_params=pltpu.CompilerParams(vmem_limit_bytes=16 << 20),
        )(*in_hbm(*weights), after)

    p_alpha, p_beta = load((project_alpha, project_beta), got_same[2])

    total = chips * rows
    spare = (m, n, w, *lines[1:], p_alpha)
    work = [
        pltpu.VMEM((2, planes * rows, LANE), F32),
        pltpu.VMEM((2 * rows, 2 * rows), BF),
    ]
    half = shape_of((planes * rows, LANE))
    other_x, *held = call(
        lambda *refs: attend_one_kernel(planes, len(spare), *refs),
        [half, shape_of((2, total, LANE)), shape_of((total, LANE)), shape_of((total, LANE)), shape_of((8, total), F32)],
        (*got_same, *got_cross, relayed, *spare),
        12,
        hidden=len(spare),
        scratch=work,
    )
    got_x = swap_plane(other_x, 1, 0)
    (own_x,) = call(
        lambda *refs: attend_two_kernel(planes, *refs), [half], tuple(held), 12, scratch=work
    )
    merged = call(merge_kernel, [shape_of((rows, 2 * LANE))] * planes, (own_x, got_x), 4)
    back = [merged[0]] + [shift(merged[d], d, 0) for d in range(1, planes)]
    gains = jnp.concatenate([gain_alpha, gain_beta])[None, :]
    att, sums = call(
        lambda *refs: collect_kernel(planes, *refs),
        [shape_of((rows, 2 * width)), shape_of((8, rows), F32)],
        (*back, gains),
        8,
    )
    all_sums = across_tp(sums)

    keep, send = call(
        lambda *refs: project_kernel(columns, *refs),
        [shape_of((2 * cap, columns))] * 2,
        (att, m, *in_hbm(residual_in), *all_sums, p_alpha, p_beta),
        12,
        scratch=[pltpu.VMEM((rows, columns), F32)],
    )
    own, send = call(
        pair_kernel,
        [shape_of((cap, columns), F32), shape_of((cap, columns))],
        (keep, swap_tp(send, 1)),
        8,
    )
    got = swap_tp(send, 2)
    e_gate, e_up, e_down = load((expert_gate, expert_up, expert_down), keep)
    settled, _ = call(
        settle_kernel,
        [shape_of((cap, columns + LANE)), shape_of((2, columns), F32)],
        (own, got, w, *lines),
        8,
    )

    def to_plane(z, x, t):
        g = t ^ (2 * (z & 1))
        return g, x, 2 * (t >> 1) + (z >> 1)

    mine = move(settled, to_plane)
    from_x, from_y = swap_plane(mine, 1, 0), swap_plane(mine, 0, 2)
    from_xy = swap_plane(from_x, 0, 2)
    near = [mine, from_x, from_y]
    far = [swap_plane(mine, 0, 1)] + [swap_plane(v, 0, 1) for v in near[1:]]
    hidden = expert_gate.shape[2]

    def experts(pieces):
        n = len(pieces) * cap
        return call(
            expert_kernel,
            [shape_of((n, 2 * width))] * 2,
            (*pieces, e_gate, e_up, e_down),
            24,
            scratch=[
                pltpu.VMEM((n, columns), BF),
                pltpu.VMEM((n, hidden), BF),
                pltpu.VMEM((n, 1), F32),
            ],
        )

    def chip(spots, targets, outs, own, got):
        kernel = lambda *refs: chip_kernel(spots, targets, *refs)
        return call(kernel, outs, (own, got), 8)

    whole, side = shape_of((4 * cap, width)), shape_of((2 * cap, width))
    near_one, far_one = experts(near + far)
    keep, to_y, to_x0, to_xy0 = chip(
        ((0, 0), (1, 0), (0, 1)),
        ((0, 0), (0, 1), (1, 0), (1, 1)),
        [shape_of(whole.shape, F32), whole, side, side],
        near_one,
        swap_plane(far_one, 0, 1),
    )
    last, _ = lax.optimization_barrier((from_xy, far_one))
    near_two, far_two = experts([last, swap_plane(last, 0, 1)])
    to_x1, to_xy1 = chip(
        ((1, 1),), ((1, 0), (1, 1)), [side, side], near_two, swap_plane(far_two, 0, 1)
    )
    got_y = swap_plane(to_y, 0, 2)
    got_x0, got_x1 = swap_plane(to_x0, 1, 0), swap_plane(to_x1, 1, 0)
    got_xy1, got_xy0 = swap_plane(to_xy0, 1, 2), swap_plane(to_xy1, 1, 2)
    second, sums = call(
        second_kernel,
        [shape_of((4 * cap, width), F32), shape_of((8, 2 * LANE), F32)],
        (keep, got_y, got_x0, got_x1, got_xy0, got_xy1, near[0], near[2], far[0], far[2]),
        8,
        scratch=[pltpu.VMEM((4 * cap, width), F32)],
    )
    all_sums = across_tp(sums)
    ends = call(
        lambda *refs: finish_kernel(columns, *refs),
        [shape_of((cap, width))] * planes,
        (second, *all_sums, jnp.stack([gain_final, bias_final])),
        8,
        scratch=[pltpu.VMEM((4 * cap, width), BF)],
    )
    home = [ends[0]] + [shift(ends[d], d, 0) for d in range(1, planes)]
    (out,) = call(place_kernel, [shape_of((rows, width))], (n, *home), 4)
    return out


def solution(mesh):
    chips, lanes = mesh.shape["sp"], mesh.shape["tp"]

    def body(*args):
        residual_in, pairs_alpha, pairs_beta = args[0], args[2], args[6]
        planes = chips // 2
        fast = (
            chips // GROUP_COUNT == 2
            and lanes == planes
            and lanes == 4
            and pairs_alpha.shape[1] == planes
            and pairs_beta.shape[1] == planes
            and pairs_alpha.shape[2] == LANE
            and pairs_beta.shape[2] == 2 * LANE
            and residual_in.shape[0] == LANE
            and args[1].shape[1] == planes * LANE
            and args[5].shape[1] == planes * LANE
        )
        if not fast:
            return general_body(*args)
        return fast_body(chips, lanes, *args)

    in_specs = (
        P("sp", "tp"),
        P("sp", "tp"),
        P("sp", "tp", None),
        P("sp", "tp"),
        P("tp"),
        P("sp", "tp"),
        P("sp", "tp", None),
        P("sp", "tp"),
        P("tp"),
        P("tp", None),
        P("tp", None),
        P("tp"),
        P("tp"),
        P("sp", None),
        P("sp", None),
        P("sp", None, "tp"),
        P("sp", None, "tp"),
        P("sp", "tp", None),
        P("tp"),
        P("tp"),
    )
    out_specs = P("sp", "tp")
    return jax.shard_map(body, mesh=mesh, in_specs=in_specs, out_specs=out_specs, check_vma=False)
```

```python
import jax
import jax.numpy as jnp
from jax import lax
from jax.experimental import pallas as pl
from jax.experimental.pallas import tpu as pltpu
from jax.sharding import PartitionSpec as P


depth_scale = 2.0**0.5
norm_eps = 1e-05


def break_block(acc, remain, queries, pairs, offsets, key_first, query_first):
    width = queries.shape[3]
    keys = pairs[:, :, :width]
    values = pairs[:, :, width:]
    length = offsets.shape[0]
    kv_heads = queries.shape[1]
    share = queries.shape[2]
    scores = jnp.einsum(
        "qhrd,khd->hrqk", queries, keys, preferred_element_type=jnp.float32
    ) * width ** (-0.5)
    scores = (
        scores + jnp.transpose(offsets.reshape(length, kv_heads, share), (1, 2, 0))[:, :, None, :]
    )
    query_pos = query_first + jnp.arange(queries.shape[0], dtype=jnp.int32)
    key_pos = key_first + jnp.arange(length, dtype=jnp.int32)
    valid = key_pos[None, :] < query_pos[:, None]
    soft = jnp.where(valid, jax.nn.softplus(scores), 0.0)
    later = lax.cumsum(soft, axis=3, reverse=True) - soft
    weights = jnp.where(
        valid, jnp.exp(jax.nn.log_sigmoid(scores) - later + remain[..., None]), 0.0
    ).astype(jnp.bfloat16)
    acc = acc + jnp.einsum("hrqk,khd->qhrd", weights, values, preferred_element_type=jnp.float32)
    return (acc, remain - jnp.sum(soft, axis=3))


def finish_norm(total, sums, gain, bias, columns):
    mean = sums[0] / columns
    var = sums[1] / columns - mean * mean
    return ((total - mean[:, None]) * lax.rsqrt(var + norm_eps)[:, None] * gain + bias).astype(
        jnp.bfloat16
    )


def general_body(
    residual_in,
    query_alpha,
    pairs_alpha,
    offset_alpha,
    gain_alpha,
    query_beta,
    pairs_beta,
    offset_beta,
    gain_beta,
    project_alpha,
    project_beta,
    gain_settle,
    bias_settle,
    expert_ids,
    route_weight,
    expert_gate,
    expert_up,
    expert_down,
    gain_final,
    bias_final,
):
    rows = residual_in.shape[0]
    mine = lax.axis_index("sp")
    count = lax.axis_size("sp")
    heads_tp = lax.axis_size("tp")
    width_alpha = pairs_alpha.shape[2] // 2
    width_beta = pairs_beta.shape[2] // 2
    grouped_alpha = query_alpha.reshape(rows, pairs_alpha.shape[1], -1, width_alpha)
    grouped_beta = query_beta.reshape(rows, pairs_beta.shape[1], -1, width_beta)
    query_first = mine * rows
    initial = (
        jnp.zeros(grouped_alpha.shape, jnp.float32),
        jnp.zeros(grouped_beta.shape, jnp.float32),
        jnp.zeros((grouped_alpha.shape[1], grouped_alpha.shape[2], rows), jnp.float32),
        jnp.zeros((grouped_beta.shape[1], grouped_beta.shape[2], rows), jnp.float32),
    )

    def visit(state, pairs, offsets, key_first):
        acc_alpha, acc_beta, rest_alpha, rest_beta = state
        acc_alpha, rest_alpha = break_block(
            acc_alpha, rest_alpha, grouped_alpha, pairs[0], offsets[0], key_first, query_first
        )
        acc_beta, rest_beta = break_block(
            acc_beta, rest_beta, grouped_beta, pairs[1], offsets[1], key_first, query_first
        )
        return (acc_alpha, acc_beta, rest_alpha, rest_beta)

    def maybe_visit(state, turn, pairs, offsets):
        return lax.cond(
            turn <= mine,
            lambda kept: visit(kept, pairs, offsets, (mine - turn) * rows),
            lambda kept: kept,
            state,
        )

    pairs_all = (
        lax.all_gather(pairs_alpha, "sp", axis=0, tiled=True),
        lax.all_gather(pairs_beta, "sp", axis=0, tiled=True),
    )
    offsets_all = (
        lax.all_gather(offset_alpha, "sp", axis=0, tiled=True),
        lax.all_gather(offset_beta, "sp", axis=0, tiled=True),
    )

    def turn_all(turn, state):
        first_row = (mine - turn) * rows
        pairs = (
            lax.dynamic_slice_in_dim(pairs_all[0], first_row, rows, 0),
            lax.dynamic_slice_in_dim(pairs_all[1], first_row, rows, 0),
        )
        offsets = (
            lax.dynamic_slice_in_dim(offsets_all[0], first_row, rows, 0),
            lax.dynamic_slice_in_dim(offsets_all[1], first_row, rows, 0),
        )
        return maybe_visit(state, turn, pairs, offsets)

    state = lax.fori_loop(0, count, turn_all, initial)
    attend_alpha = state[0].reshape(rows, -1)
    attend_beta = state[1].reshape(rows, -1)
    squares = lax.psum(
        (jnp.sum(attend_alpha * attend_alpha, axis=1), jnp.sum(attend_beta * attend_beta, axis=1)),
        "tp",
    )
    scale_alpha = lax.rsqrt(squares[0] / (attend_alpha.shape[1] * heads_tp) + norm_eps)
    scale_beta = lax.rsqrt(squares[1] / (attend_beta.shape[1] * heads_tp) + norm_eps)
    normed_alpha = (attend_alpha * scale_alpha[:, None] * gain_alpha).astype(jnp.bfloat16)
    normed_beta = (attend_beta * scale_beta[:, None] * gain_beta).astype(jnp.bfloat16)
    term = jnp.dot(normed_alpha, project_alpha, preferred_element_type=jnp.float32) + jnp.dot(
        normed_beta, project_beta, preferred_element_type=jnp.float32
    )
    mixed = lax.psum_scatter(term.astype(jnp.bfloat16), "tp", scatter_dimension=1, tiled=True)
    columns = residual_in.shape[1] * heads_tp
    first = depth_scale * residual_in.astype(jnp.float32) + mixed.astype(jnp.float32)
    sums_one = lax.psum((jnp.sum(first, axis=1), jnp.sum(first * first, axis=1)), "tp")
    settled = finish_norm(first, sums_one, gain_settle, bias_settle, columns)
    cap = 3 * rows // count
    flat_ids = expert_ids.reshape(2 * rows)
    onehot = (flat_ids[:, None] == jnp.arange(count, dtype=jnp.int32)[None, :]).astype(jnp.int32)
    before = jnp.cumsum(onehot, axis=0, dtype=jnp.int32) - onehot
    slot = jnp.sum(before * onehot, axis=1, dtype=jnp.int32)
    place = flat_ids * cap + slot
    hit = place[None, :] == jnp.arange(count * cap, dtype=jnp.int32)[:, None]
    owner = jnp.arange(2 * rows, dtype=jnp.int32) // 2
    source = jnp.sum(jnp.where(hit, owner[None, :], 0), axis=1, dtype=jnp.int32)
    filled = jnp.any(hit, axis=1)
    gate_local = expert_gate[0]
    up_local = expert_up[0]
    send = jnp.where(filled[:, None], settled[source], jnp.zeros((), jnp.bfloat16)).reshape(
        count, cap, -1
    )
    arrived = lax.all_to_all(send, "sp", split_axis=0, concat_axis=0, tiled=True)
    piece = lax.all_gather(arrived, "tp", axis=2, tiled=True)
    flat = piece.reshape(-1, piece.shape[2])
    gate = jnp.dot(flat, gate_local, preferred_element_type=jnp.float32)
    up = jnp.dot(flat, up_local, preferred_element_type=jnp.float32)
    hidden = (jax.nn.silu(gate) * up).astype(jnp.bfloat16)
    partial_value = jnp.dot(hidden, expert_down[0], preferred_element_type=jnp.float32).reshape(
        count, cap, -1
    )
    summed = lax.psum_scatter(
        partial_value.astype(jnp.bfloat16), "tp", scatter_dimension=2, tiled=True
    )
    back = lax.all_to_all(summed, "sp", split_axis=0, concat_axis=0, tiled=True).reshape(
        count * cap, -1
    )
    picked = back[place].reshape(rows, 2, -1).astype(jnp.float32)
    routed = route_weight[:, 0:1] * picked[:, 0] + route_weight[:, 1:2] * picked[:, 1]
    second = depth_scale * settled.astype(jnp.float32) + routed
    sums_two = lax.psum((jnp.sum(second, axis=1), jnp.sum(second * second, axis=1)), "tp")
    return finish_norm(second, sums_two, gain_final, bias_final, columns)


GROUP_COUNT = 4
LANE = 128
BF = jnp.bfloat16
F32 = jnp.float32
LOG2E = 1.4426950408889634


def dot(a, b, dims=((1,), (0,))):
    return lax.dot_general(a, b, (dims, ((), ())), preferred_element_type=F32)


def thirds(v):
    hi = v.astype(BF).astype(F32)
    mid = (v - hi).astype(BF).astype(F32)
    return hi, mid, v - hi - mid


def iota(shape, dim):
    return lax.broadcasted_iota(jnp.int32, shape, dim)


def call(kernel, outs, args, vmem, scratch=(), hidden=0):
    local = pl.BlockSpec(memory_space=pltpu.VMEM)
    spare = pl.BlockSpec(memory_space=pl.ANY)
    return pl.pallas_call(
        kernel,
        out_shape=outs,
        in_specs=[local] * (len(args) - hidden) + [spare] * hidden,
        out_specs=[local] * len(outs),
        scratch_shapes=list(scratch),
        compiler_params=pltpu.CompilerParams(vmem_limit_bytes=vmem << 20),
    )(*args)


def spot():
    sp = lax.axis_index("sp")
    tp = lax.axis_index("tp")
    return sp // 2, sp % 2, tp


def in_hbm(*values):
    return tuple(pltpu.with_memory_space_constraint(v, pltpu.HBM) for v in values)


def shape_of(shape, dtype=BF):
    return jax.ShapeDtypeStruct(shape, dtype)


def route_kernel(cap, ids, weight, *refs):
    m_out, n_out, w_out = refs[-3:]
    z, _, t = spot()
    rows = ids.shape[1]
    first = iota((rows, rows), 0)
    second = iota((rows, rows), 1)

    def column(line):
        return jnp.sum(jnp.where(first == second, line, 0), axis=1, keepdims=True)

    grow = lax.shift_right_logical(ids[0:1, :], 1)
    gcol = column(grow)
    same = gcol == grow
    slot_col = jnp.sum(jnp.where(same & (second < first), 1, 0), axis=1, keepdims=True)
    slot_row = jnp.sum(jnp.where(same & (first < second), 1, 0), axis=0, keepdims=True)
    away = (grow ^ (2 * (z & 1))) ^ t
    block = 2 * (away & 1) + lax.shift_right_logical(away, 1)
    m = jnp.where(iota((4 * cap, rows), 0) == block * cap + slot_row, 1.0, 0.0).astype(BF)
    m_out[...] = m
    place = ((z + 4 - gcol) & 3) * cap + slot_col
    n_out[...] = jnp.where(iota((rows, 4 * cap), 1) == place, 1.0, 0.0).astype(BF)
    even = (ids[0:1, :] & 1) == 0
    w_even = column(jnp.where(even, weight[0:1, :], weight[1:2, :]))
    w_odd = column(jnp.where(even, weight[1:2, :], weight[0:1, :]))
    lane = iota((rows, LANE), 1)
    table = jnp.zeros((rows, LANE), F32)
    for k, part in enumerate(thirds(w_even) + thirds(w_odd)):
        table = jnp.where(lane == k, part, table)
    w_out[...] = dot(m[:cap], table.astype(BF)).astype(BF)


def pack_kernel(side, qa, ka, qb, kb, offs_a, offs_b, *outs):
    z, x, _ = spot()
    rows = qa.shape[0]
    planes = qa.shape[1] // LANE

    def offset_rows(ref, values):
        parts = []
        for v in values:
            parts += list(thirds(v))
        parts += [jnp.zeros((1, LANE), F32)] * (8 - len(parts))
        block = jnp.concatenate(parts, axis=0).astype(BF)
        for k in range(ref.shape[1] // LANE):
            ref[pl.ds(rows, 8), k * LANE : (k + 1) * LANE] = block

    all_a = ka[...].astype(F32)
    all_b = kb[...].astype(F32)
    for u in range(planes):
        d = (u + planes - z) % planes
        cols = slice(u * LANE, (u + 1) * LANE)
        kv = all_a[:, u, :].astype(BF)
        kv_beta = all_b[:, u, :].astype(BF)
        for k, ref in enumerate(outs):

            @pl.when((d == k) & (x == side))
            def _():
                ref[0:rows, 0:LANE] = qa[:, cols]
                ref[0:rows, LANE : 2 * LANE] = kv
                offset_rows(ref, [offs_a[2 * u : 2 * u + 1, :], offs_a[2 * u + 1 : 2 * u + 2, :]])

            @pl.when((d == k) & (x != side))
            def _():
                ref[0:rows, 0:LANE] = qb[:, cols]
                ref[0:rows, LANE : 2 * LANE] = kv_beta[:, 0:LANE]
                offset_rows(ref, [offs_b[u : u + 1, :]])

            if side == 0:

                @pl.when(d == k)
                def _():
                    ref[0:rows, 2 * LANE :] = kv_beta[:, LANE:]


def relay_kernel(*refs):
    out = refs[-1]
    rows = out.shape[0] // (len(refs) - 1)
    for d, ref in enumerate(refs[:-1]):
        out[d * rows : (d + 1) * rows, :] = ref[0:rows, 2 * LANE :]


def gather_kernel(planes, same, cross, relayed, q_s, k_s, v_s, off_s):
    z, x, _ = spot()
    rows = k_s.shape[0] // (2 * planes)
    half = LANE // 2
    low = iota((rows, LANE), 1) < half
    for d in range(planes):
        for ref, other in ((same[d], x), (cross[d], 1 - x)):
            p = (z + planes - d) % planes
            at = pl.ds(pl.multiple_of((2 * p + other) * rows, rows), rows)
            by_x = pl.ds(pl.multiple_of((planes * other + p) * rows, rows), rows)
            q = ref[0:rows, 0:LANE]
            zero = jnp.zeros_like(q)
            q_s[0, by_x, :] = jnp.where(low | (x != 0), q, zero)
            q_s[1, by_x, :] = jnp.where(low, zero, q)
            kv = ref[0:rows, LANE : 2 * LANE]
            turned = jnp.concatenate([kv[:, half:], kv[:, :half]], axis=1)
            values = relayed[d * rows : (d + 1) * rows, :] if ref is cross[d] else ref[0:rows, 2 * LANE :]
            k_s[at, :] = jnp.where(low | (x != 0), kv, turned)
            v_s[at, :] = jnp.where(x != 0, values, jnp.where(low, turned, kv))
            lines = ref[pl.ds(rows, 8), 0:LANE].astype(F32)
            for h in range(2):
                off_s[h : h + 1, at] = LOG2E * jnp.sum(lines[3 * h : 3 * h + 3], axis=0, keepdims=True)


def attend_half(planes, side, q_s, k_s, v_s, off_s, out, acc_s, tri_s):
    z, x, _ = spot()
    rows = k_s.shape[0] // (2 * planes)
    tile = 2 * rows
    low = iota((rows, LANE), 1) < LANE // 2
    ti = iota((tile, tile), 0)
    tj = iota((tile, tile), 1)
    tri_s[...] = jnp.where(ti > tj, 1.0, 0.0).astype(BF)
    valid = (tj < ti + side * rows) | (ti >= rows)
    scale = jnp.where(x == 0, (LANE // 2) ** (-0.5) * LOG2E, LANE ** (-0.5) * LOG2E).astype(F32)
    base = side * (planes * rows)

    def run(heads):
        tasks = []
        for j in range(planes - 1, -1, -1):
            for first in range(j, planes, 2):
                tasks += [(h, j, first, min(2, planes - first)) for h in range(heads)]
        rest = {}

        def product(task):
            h, j, first, count = task
            cols = slice(j * tile, (j + 1) * tile)
            at = pl.ds(pl.multiple_of(base + first * rows, rows), count * rows)
            return dot(q_s[h, at, :], k_s[cols, :], ((1,), (1,)))

        def suffix(task, s):
            h, j, first, count = task
            s = s * scale + off_s[h : h + 1, j * tile : (j + 1) * tile]
            top = jnp.minimum(s, 64.0)
            take = top - jnp.log2(1.0 + jnp.exp2(top))
            soft = s - take
            if first == j:
                soft = jnp.where(valid[: count * rows], soft, 0.0)
            soft = soft.astype(BF)
            after = dot(soft, tri_s[...])
            return take, after, soft[:, 0:1].astype(F32)

        def gather(task, take, after, own):
            h, j, first, count = task
            fresh = first == j
            blocks = range(first, first + count)
            zero = jnp.zeros((rows, 1), F32)
            before = [rest.get((h, i), zero) for i in blocks]
            before = before[0] if count == 1 else jnp.concatenate(before, axis=0)
            w = jnp.exp2(take - (after + before))
            if fresh:
                w = jnp.where(valid[: count * rows], w, 0.0)
            part = dot(w.astype(BF), v_s[j * tile : (j + 1) * tile, :])
            total = before + after[:, 0:1] + own
            for k, i in enumerate(blocks):
                at = slice(i * rows, (i + 1) * rows)
                piece = part[k * rows : (k + 1) * rows]
                acc_s[h, at, :] = piece if i == j else acc_s[h, at, :] + piece
                rest[(h, i)] = total[k * rows : (k + 1) * rows]

        count = len(tasks)
        ahead, middle = {}, {}
        for n in range(count + 2):
            if n < count:
                ahead[n] = product(tasks[n])
            if 0 <= n - 1 < count:
                middle[n - 1] = suffix(tasks[n - 1], ahead.pop(n - 1))
            if 0 <= n - 2:
                gather(tasks[n - 2], *middle.pop(n - 2))

    @pl.when(x == 0)
    def _():
        run(2)

    @pl.when(x != 0)
    def _():
        run(1)

    for d in range(planes):
        at = pl.ds(pl.multiple_of(((z + d) % planes) * rows, rows), rows)
        value = jnp.where(low | (x != 0), acc_s[0, at, :], acc_s[1, at, :])
        out[d * rows : (d + 1) * rows, :] = value.astype(BF)


def attend_one_kernel(planes, *refs):
    same, cross = refs[:planes], refs[planes : 2 * planes]
    refs = refs[2 * planes :]
    out, *held = refs[1:6]
    gather_kernel(planes, same, cross, refs[0], *held)
    side = 1 - lax.axis_index("sp") % 2
    attend_half(planes, side, *held, out, *refs[6:])


def attend_two_kernel(planes, *refs):
    attend_half(planes, lax.axis_index("sp") % 2, *refs)


def merge_kernel(own, got, *outs):
    _, x, _ = spot()
    rows = own.shape[0] // len(outs)
    for d, ref in enumerate(outs):
        at = slice(d * rows, (d + 1) * rows)
        ref[:, pl.ds(pl.multiple_of(x * LANE, LANE), LANE)] = own[at]
        ref[:, pl.ds(pl.multiple_of((1 - x) * LANE, LANE), LANE)] = got[at]


def collect_kernel(planes, *refs):
    parts = refs[:planes]
    gains, out, sums = refs[planes:]
    z, _, _ = spot()
    width = planes * LANE
    lane = LANE
    for d in range(planes):
        u = (z + planes - d) % planes
        for k in range(2):
            at = pl.ds(pl.multiple_of(k * width + u * lane, lane), lane)
            out[:, at] = parts[d][:, k * lane : (k + 1) * lane]
    whole = out[...].astype(F32)
    for k in range(2):
        part = whole[:, k * width : (k + 1) * width]
        sums[k : k + 1, :] = row_sums(part * part)
    sums[2:8, :] = jnp.zeros((6, sums.shape[1]), F32)
    out[...] = (whole * gains[0:1, :]).astype(BF)


def project_kernel(columns, att, m, resid, s0, s1, s2, s3, pa, pb, keep, send, t_s):
    rows, width = resid.shape
    total = s0[0:2, :] + s1[0:2, :] + s2[0:2, :] + s3[0:2, :]
    factor = lax.rsqrt(total / columns + norm_eps)
    eye = iota((rows, rows), 0) == iota((rows, rows), 1)
    f_a = jnp.sum(jnp.where(eye, factor[0:1], 0.0), axis=1, keepdims=True)
    f_b = jnp.sum(jnp.where(eye, factor[1:2], 0.0), axis=1, keepdims=True)
    for k in range(columns // width):
        at = slice(k * width, (k + 1) * width)
        t_s[:, at] = dot(att[:, :width], pa[:, at]) * f_a + dot(att[:, width:], pb[:, at]) * f_b
    own = pl.ds(pl.multiple_of(lax.axis_index("tp") * width, LANE), width)
    t_s[:, own] = t_s[:, own] + depth_scale * resid[...].astype(F32)
    mid = keep.shape[0]
    for k in range(columns // width):
        at = slice(k * width, (k + 1) * width)
        moved = dot(m[...], t_s[:, at].astype(BF)).astype(BF)
        keep[:, at] = moved[:mid]
        send[:, at] = moved[mid:]


def pair_kernel(keep, got, own, send):
    n = own.shape[0]
    total = keep[...].astype(F32) + got[...].astype(F32)
    own[...] = total[:n]
    send[...] = total[n:].astype(BF)


def settle_kernel(own, got, w, l0, l1, l2, l3, out, lines):
    _, _, t = spot()
    width = l0.shape[1]
    for k, ref in enumerate((l0, l1, l2, l3)):
        lines[:, pl.ds(pl.multiple_of((t ^ k) * width, LANE), width)] = ref[...]
    columns = lines.shape[1]
    first = own[...] + got[...].astype(F32)
    out[:, 0:columns] = row_norm(first, lines[0:1, :], lines[1:2, :])
    out[:, columns : columns + LANE] = w[...]


def row_sums(v):
    n = v.shape[0]
    column = jnp.sum(v, axis=1, keepdims=True)
    eye = iota((n, n), 0) == iota((n, n), 1)
    return jnp.sum(jnp.where(eye, column, 0.0), axis=0, keepdims=True)


def row_norm(total, gain, bias):
    columns = total.shape[1]
    mean = jnp.sum(total, axis=1, keepdims=True) / columns
    var = jnp.sum(total * total, axis=1, keepdims=True) / columns - mean * mean
    return ((total - mean) * lax.rsqrt(var + norm_eps) * gain + bias).astype(BF)


def expert_kernel(*refs):
    gate, up, down, near, far, x_s, h_s, w_s = refs[-8:]
    n = refs[0].shape[0]
    count = x_s.shape[0] // n
    columns = x_s.shape[1]
    odd = lax.axis_index("sp") % 2 != 0
    _, _, t = spot()
    for k, piece in enumerate(refs[:count]):
        at = slice(k * n, (k + 1) * n)
        x_s[at, :] = piece[:, 0:columns]
        w = piece[:, columns : columns + LANE].astype(F32)
        even_w = w[:, 0:1] + w[:, 1:2] + w[:, 2:3]
        odd_w = w[:, 3:4] + w[:, 4:5] + w[:, 5:6]
        w_s[at, :] = jnp.where(odd, odd_w, even_w)

    x = x_s[...]
    chunk = 2 * LANE
    chunks = h_s.shape[1] // chunk
    ahead = None
    for k in range(chunks + 1):
        this = None
        if k < chunks:
            at = slice(k * chunk, (k + 1) * chunk)
            this = dot(x, gate[0, :, at]), dot(x, up[0, :, at])
        if ahead is not None:
            g, u = ahead
            h_s[:, (k - 1) * chunk : k * chunk] = (g / (1.0 + jnp.exp(-g)) * u).astype(BF)
        ahead = this

    mid = count // 2 * n
    width = near.shape[1] // 2
    for k in range(2):
        cols = slice(k * width, (k + 1) * width)
        at = pl.ds(pl.multiple_of((t ^ (2 * k + 1)) * width, LANE), width)
        value = (dot(h_s[...], down[0, :, at]) * w_s[...]).astype(BF)
        far[0:mid, cols] = value[mid:]
        far[mid:, cols] = value[:mid]
        at = pl.ds(pl.multiple_of((t ^ (2 * k)) * width, LANE), width)
        near[:, cols] = (dot(h_s[...], down[0, :, at]) * w_s[...]).astype(BF)


def chip_kernel(spots, targets, near, got, *refs):
    width = near.shape[1] // 2
    count = len(spots)
    n = near.shape[0] // (2 * count)
    for dc in range(2):
        for k, (dx, dy) in enumerate(spots):
            rows = slice((count * dc + k) * n, (count * dc + k + 1) * n)
            for ry in range(2):
                ref = refs[targets.index((dx, ry))]
                cols = slice(ry * width, (ry + 1) * width)
                total = near[rows, cols].astype(F32) + got[rows, cols].astype(F32)
                q = 2 * dc + (dy ^ ry) if ref.shape[0] == 4 * n else dc
                ref[q * n : (q + 1) * n, :] = total.astype(ref.dtype)


def second_kernel(keep, gy, gx0, gx1, gxy0, gxy1, s0, s1, s2, s3, second, sums, routed_s):
    z, _, t = spot()
    n = s0.shape[0]
    width = keep.shape[1]
    at = pl.ds(pl.multiple_of(t * width, LANE), width)
    for q, ref in enumerate((s0, s1, s2, s3)):
        rows = slice(q * n, (q + 1) * n)
        side = slice((q >> 1) * n, ((q >> 1) + 1) * n)
        routed = keep[rows, :] + gy[rows, :].astype(F32)
        for part in (gx1, gxy1) if q & 1 else (gx0, gxy0):
            routed = routed + part[side, :].astype(F32)
        routed_s[rows, :] = routed + depth_scale * ref[:, at].astype(F32)
    for k in range(4):
        dc = (k >> 1) ^ (t & 1)
        dy = ((k & 1) ^ lax.shift_right_logical(z, 1)) ^ lax.shift_right_logical(t, 1)
        start = pl.multiple_of((2 * dc + dy) * n, 16)
        second[k * n : (k + 1) * n, :] = routed_s[pl.ds(start, n), :]
    value = second[...]
    for k, part in enumerate((value, value * value)):
        sums[k : k + 1, 0 : 4 * n] = row_sums(part)


def finish_kernel(columns, second, c0, c1, c2, c3, lines, f0, f1, f2, f3, all_s):
    z, _, _ = spot()
    n = f0.shape[0]
    total = c0[0:2, 0 : 4 * n] + c1[0:2, 0 : 4 * n] + c2[0:2, 0 : 4 * n] + c3[0:2, 0 : 4 * n]
    mean = total[0:1] / columns
    scale = lax.rsqrt(total[1:2] / columns - mean * mean + norm_eps)
    eye = iota((4 * n, 4 * n), 0) == iota((4 * n, 4 * n), 1)
    mean = jnp.sum(jnp.where(eye, mean, 0.0), axis=1, keepdims=True)
    scale = jnp.sum(jnp.where(eye, scale, 0.0), axis=1, keepdims=True)
    all_s[...] = ((second[...] - mean) * scale * lines[0:1, :] + lines[1:2, :]).astype(BF)
    for d, ref in enumerate((f0, f1, f2, f3)):
        start = pl.multiple_of(((z + d) & 3) * n, 16)
        ref[...] = all_s[pl.ds(start, n), :]


def load_kernel(*refs):
    count = (len(refs) - 1) // 2
    sems = refs[-1]
    copies = [
        pltpu.make_async_copy(refs[k], refs[count + k], sems.at[k]) for k in range(count)
    ]
    for copy in copies:
        copy.start()
    for copy in copies:
        copy.wait()


def place_kernel(n, f0, f1, f2, f3, out):
    total = dot(n[...], jnp.concatenate([f0[...], f1[...], f2[...], f3[...]], axis=0))
    out[...] = total.astype(BF)


def fast_body(
    chips,
    lanes,
    residual_in,
    query_alpha,
    pairs_alpha,
    offset_alpha,
    gain_alpha,
    query_beta,
    pairs_beta,
    offset_beta,
    gain_beta,
    project_alpha,
    project_beta,
    gain_settle,
    bias_settle,
    expert_ids,
    route_weight,
    expert_gate,
    expert_up,
    expert_down,
    gain_final,
    bias_final,
):
    rows, width = residual_in.shape
    planes = chips // 2
    columns = width * lanes
    cap = 3 * rows // chips

    def move(v, dest):
        perm = []
        for a in range(chips * lanes):
            s, t = divmod(a, lanes)
            to = dest(s // 2, s % 2, t)
            if to is not None:
                perm.append((a, (to[0] * 2 + to[1]) * lanes + to[2]))
        return lax.ppermute(v, ("sp", "tp"), perm)

    def shift(v, d, flip):
        return move(v, lambda z, x, t: ((z + d) % planes, x ^ flip, t))

    def swap_tp(v, k):
        return move(v, lambda z, x, t: (z, x, t ^ k))

    def across_tp(v):
        return v, swap_tp(v, 1), swap_tp(v, 2), swap_tp(v, 3)

    def swap_plane(v, dx, k):
        return move(v, lambda z, x, t: (z, x ^ dx, t ^ k))

    inputs = in_hbm(
        query_alpha,
        pairs_alpha,
        query_beta,
        pairs_beta,
        jnp.transpose(offset_alpha),
        jnp.transpose(offset_beta),
    )
    same, cross = (
        call(
            lambda *refs: pack_kernel(flip, *refs),
            [shape_of((rows + 8, (3 - flip) * LANE))] * planes,
            inputs,
            12,
        )
        for flip in range(2)
    )
    got_same, got_cross = [same[0]] + [None] * (planes - 1), [None] * planes
    for d in (2, 1, 3):
        got_same[d] = shift(same[d], d, 0)
    for d in (2, 1, 3, 0):
        got_cross[d] = shift(cross[d], d, 1)
    (values,) = call(relay_kernel, [shape_of((planes * rows, LANE))], got_same, 4)
    relayed = swap_plane(values, 1, 0)

    own_lines = jnp.stack([gain_settle, bias_settle])
    lines = [own_lines] + [swap_tp(own_lines, k) for k in range(1, 4)]

    def load(weights, after):
        count = len(weights)
        anywhere = pl.BlockSpec(memory_space=pl.ANY)
        return pl.pallas_call(
            lambda *refs: load_kernel(*refs[:count], *refs[count + 1 :]),
            out_shape=[shape_of(v.shape) for v in weights],
            in_specs=[anywhere] * (count + 1),
            out_specs=[pl.BlockSpec(memory_space=pltpu.VMEM)] * count,
            scratch_shapes=[pltpu.SemaphoreType.DMA((count,))],
            compiler_params=pltpu.CompilerParams(vmem_limit_bytes=16 << 20),
        )(*in_hbm(*weights), after)

    total = chips * rows
    work = [
        pltpu.VMEM((2, planes * rows, LANE), F32),
        pltpu.VMEM((2 * rows, 2 * rows), BF),
    ]
    half = shape_of((planes * rows, LANE))
    other_x, *held = call(
        lambda *refs: attend_one_kernel(planes, *refs),
        [half, shape_of((2, total, LANE)), shape_of((total, LANE)), shape_of((total, LANE)), shape_of((8, total), F32)],
        (*got_same, *got_cross, relayed),
        12,
        scratch=work,
    )
    got_x = swap_plane(other_x, 1, 0)
    (own_x,) = call(
        lambda *refs: attend_two_kernel(planes, *refs), [half], tuple(held), 12, scratch=work
    )
    merged = call(merge_kernel, [shape_of((rows, 2 * LANE))] * planes, (own_x, got_x), 4)

    def to_planes(pieces):
        got = [pieces[0]]
        for d in range(1, planes):
            got.append(shift(pieces[d], d, 0))
        return got

    back = to_planes(merged)
    p_alpha, p_beta = load((project_alpha, project_beta), own_x)
    m, n, w = call(
        lambda *refs: route_kernel(cap, *refs),
        [shape_of((4 * cap, rows)), shape_of((rows, 4 * cap)), shape_of((cap, LANE))],
        (*in_hbm(jnp.transpose(expert_ids), jnp.transpose(route_weight)), own_x),
        8,
        hidden=1,
    )
    gains = jnp.concatenate([gain_alpha, gain_beta])[None, :]
    att, sums = call(
        lambda *refs: collect_kernel(planes, *refs),
        [shape_of((rows, 2 * width)), shape_of((8, rows), F32)],
        (*back, gains),
        8,
    )
    all_sums = across_tp(sums)

    keep, send = call(
        lambda *refs: project_kernel(columns, *refs),
        [shape_of((2 * cap, columns))] * 2,
        (att, m, *in_hbm(residual_in), *all_sums, p_alpha, p_beta),
        12,
        scratch=[pltpu.VMEM((rows, columns), F32)],
    )
    own, send = call(
        pair_kernel,
        [shape_of((cap, columns), F32), shape_of((cap, columns))],
        (keep, swap_tp(send, 1)),
        8,
    )
    got = swap_tp(send, 2)
    e_gate, e_up = load((expert_gate, expert_up), keep)
    settled, all_lines = call(
        settle_kernel,
        [shape_of((cap, columns + LANE)), shape_of((2, columns), F32)],
        (own, got, w, *lines),
        8,
    )

    def to_plane(z, x, t):
        g = t ^ (2 * (z & 1))
        return g, x, 2 * (t >> 1) + (z >> 1)

    mine = move(settled, to_plane)
    (e_down,) = load((expert_down,), all_lines)
    from_x, from_y = swap_plane(mine, 1, 0), swap_plane(mine, 0, 2)
    from_xy = swap_plane(from_x, 0, 2)
    near = [mine, from_x, from_y]
    far = [swap_plane(mine, 0, 1)] + [swap_plane(v, 0, 1) for v in near[1:]]
    hidden = expert_gate.shape[2]

    def experts(pieces):
        n = len(pieces) * cap
        return call(
            expert_kernel,
            [shape_of((n, 2 * width))] * 2,
            (*pieces, e_gate, e_up, e_down),
            24,
            scratch=[
                pltpu.VMEM((n, columns), BF),
                pltpu.VMEM((n, hidden), BF),
                pltpu.VMEM((n, 1), F32),
            ],
        )

    def chip(spots, targets, outs, own, got):
        kernel = lambda *refs: chip_kernel(spots, targets, *refs)
        return call(kernel, outs, (own, got), 8)

    whole, side = shape_of((4 * cap, width)), shape_of((2 * cap, width))
    near_one, far_one = experts(near + far)
    keep, to_y, to_x0, to_xy0 = chip(
        ((0, 0), (1, 0), (0, 1)),
        ((0, 0), (0, 1), (1, 0), (1, 1)),
        [shape_of(whole.shape, F32), whole, side, side],
        near_one,
        swap_plane(far_one, 0, 1),
    )
    last, _ = lax.optimization_barrier((from_xy, far_one))
    near_two, far_two = experts([last, swap_plane(last, 0, 1)])
    to_x1, to_xy1 = chip(
        ((1, 1),), ((1, 0), (1, 1)), [side, side], near_two, swap_plane(far_two, 0, 1)
    )
    got_y = swap_plane(to_y, 0, 2)
    got_x0, got_x1 = swap_plane(to_x0, 1, 0), swap_plane(to_x1, 1, 0)
    got_xy1, got_xy0 = swap_plane(to_xy0, 1, 2), swap_plane(to_xy1, 1, 2)
    second, sums = call(
        second_kernel,
        [shape_of((4 * cap, width), F32), shape_of((8, 2 * LANE), F32)],
        (keep, got_y, got_x0, got_x1, got_xy0, got_xy1, near[0], near[2], far[0], far[2]),
        8,
        scratch=[pltpu.VMEM((4 * cap, width), F32)],
    )
    all_sums = across_tp(sums)
    ends = call(
        lambda *refs: finish_kernel(columns, *refs),
        [shape_of((cap, width))] * planes,
        (second, *all_sums, jnp.stack([gain_final, bias_final])),
        8,
        scratch=[pltpu.VMEM((4 * cap, width), BF)],
    )
    home = to_planes(ends)
    (out,) = call(place_kernel, [shape_of((rows, width))], (n, *home), 4)
    return out


def solution(mesh):
    chips, lanes = mesh.shape["sp"], mesh.shape["tp"]

    def body(*args):
        residual_in, pairs_alpha, pairs_beta = args[0], args[2], args[6]
        planes = chips // 2
        fast = (
            chips // GROUP_COUNT == 2
            and lanes == planes
            and lanes == 4
            and pairs_alpha.shape[1] == planes
            and pairs_beta.shape[1] == planes
            and pairs_alpha.shape[2] == LANE
            and pairs_beta.shape[2] == 2 * LANE
            and residual_in.shape[0] == LANE
            and args[1].shape[1] == planes * LANE
            and args[5].shape[1] == planes * LANE
        )
        if not fast:
            return general_body(*args)
        return fast_body(chips, lanes, *args)

    in_specs = (
        P("sp", "tp"),
        P("sp", "tp"),
        P("sp", "tp", None),
        P("sp", "tp"),
        P("tp"),
        P("sp", "tp"),
        P("sp", "tp", None),
        P("sp", "tp"),
        P("tp"),
        P("tp", None),
        P("tp", None),
        P("tp"),
        P("tp"),
        P("sp", None),
        P("sp", None),
        P("sp", None, "tp"),
        P("sp", None, "tp"),
        P("sp", "tp", None),
        P("tp"),
        P("tp"),
    )
    out_specs = P("sp", "tp")
    return jax.shard_map(body, mesh=mesh, in_specs=in_specs, out_specs=out_specs, check_vma=False)
```
